512 devices in a mesh: fs: 16 (over y, x), tp: 32 (over z, core).
Axes of the slice: x: 4, y: 4, z: 16, core: 2. Of those that a mesh axis runs over, the one named last changes fastest.
Arguments:
- tokens: bfloat16 [16384, 2048], P(('fs', 'tp')), may hold values from -6 to 6
- norm_gain: float32 [2048], P('fs'), may hold values from 0.1 to 1.9
- gate_master: float32 [2048, 8192], P('fs', 'tp'), may hold values from -0.125 to 0.125
- up_master: float32 [2048, 8192], P('fs', 'tp'), may hold values from -0.125 to 0.125
- down_master: float32 [2048, 8192], P('fs', 'tp'), may hold values from -0.125 to 0.125
Outputs:
- mixed: bfloat16 [16384, 2048], P(('fs', 'tp'))
- gate_ready: bfloat16 [2048, 8192], P(None, 'tp')
- up_ready: bfloat16 [2048, 8192], P(None, 'tp')
- down_ready: bfloat16 [2048, 8192], P(None, 'tp')
The draws below stay inside these ranges and needn't reach their ends.
All inputs are finite; a program needn't handle non-finite values.
Results may differ from the reference program's by a relative error of at most 0.0095.
Values may be sent and summed in bfloat16 or wider, within the bound.
No kernel may reach another device: no remote copies, remote signals or barrier semaphores. Data moves between devices by JAX's collectives and lax.ppermute only.
A program may use at most 64 MiB of HBM per device.

```python
import jax
import jax.numpy as jnp
from jax import lax

D = 2048
FF = 8192
TOKENS = 16384
N_TP = 32


def spiked(drawn, stream_key, source, target, blocks, factor):
    owner, partner = [(jnp.arange(drawn.shape[position]) // (drawn.shape[position] // blocks)).reshape([-1 if axis == position else 1 for axis in range(drawn.ndim)]) for position in (source, target)]
    chosen = jax.random.permutation(stream_key, blocks)[partner]
    strong = (owner == chosen) | (owner == (partner + blocks // 2) % blocks)
    return jnp.where(strong, factor * drawn, drawn)


def level_of(rng, shape, shards, low, high):
    loudness, own = 1.0, jax.random.fold_in(rng, 6)
    for dim, shards_of in shards:
        heights = jnp.exp(jax.random.uniform(jax.random.fold_in(own, dim), (shards_of,), jnp.float32, low / len(shards), high / len(shards)))
        loudness = loudness * jnp.repeat(heights, shape[dim] // shards_of).reshape([-1 if axis == dim else 1 for axis in range(len(shape))])
    return loudness


def centred(key, dims, spread, limit, cuts=(), dtype=jnp.bfloat16):
    drawn = spread * jax.random.normal(key, dims, jnp.float32)
    if cuts:
        drawn = drawn * level_of(key, dims, cuts, -0.22, 0.18)
    return jnp.clip(drawn, -limit, limit).astype(dtype)


def heavy_noise(key, dims, deviation, bound, split, heavy, held_as=jnp.bfloat16):
    drawn = deviation * jax.random.normal(key, dims, jnp.float32)
    if split:
        drawn = drawn * level_of(key, dims, split, -0.22, 0.18)
    return jnp.clip(spiked(drawn, jax.random.fold_in(key, 3), *heavy), -bound, bound).astype(held_as)


def setup_inputs(seed: int = 0) -> dict:
    key_of = jax.random.split(jax.random.key(seed), 6)
    tokens = centred(key_of[0], (TOKENS, D), 1.0, 6.0, ((0, 512),))
    norm_gain = jnp.clip(1.0 + 0.18 * jax.random.normal(key_of[1], (D,), jnp.float32), 0.1, 1.9)
    gate_master = centred(key_of[2], (D, FF), D ** -0.5, 0.125, ((0, 16), (1, 32)), jnp.float32)
    up_master = centred(key_of[3], (D, FF), D ** -0.5, 0.125, ((0, 16), (1, 32)), jnp.float32)
    down_master = heavy_noise(key_of[4], (D, FF), FF ** -0.5, 0.125, ((0, 16), (1, 32)), (1, 0, 32, 2.75), jnp.float32)
    return {"tokens": tokens, "norm_gain": norm_gain, "gate_master": gate_master, "up_master": up_master, "down_master": down_master}


def reference(tokens, norm_gain, gate_master, up_master, down_master):
    gate_ready = (norm_gain[:, None] * gate_master).astype(jnp.bfloat16)
    up_ready = (norm_gain[:, None] * up_master).astype(jnp.bfloat16)
    down_ready = down_master.astype(jnp.bfloat16)
    tokens_wide = tokens.astype(jnp.float32)
    row_scale = lax.rsqrt(lax.optimization_barrier(jnp.mean(tokens_wide * tokens_wide, axis=1, keepdims=True)) + 1e-06)
    gate_proj = row_scale * jnp.dot(tokens, gate_ready, preferred_element_type=jnp.float32)
    up_proj = row_scale * jnp.dot(tokens, up_ready, preferred_element_type=jnp.float32)
    hidden = (jax.nn.silu(gate_proj) * up_proj).astype(jnp.bfloat16)
    block_width = FF // N_TP
    summed = jnp.zeros((tokens.shape[0], tokens.shape[1]), jnp.float32)
    for column_block in range(N_TP):
        lower = column_block * block_width
        partial_value = lax.dot_general(hidden[:, lower:lower + block_width], down_ready[:, lower:lower + block_width], (((1,), (1,)), ((), ())), preferred_element_type=jnp.float32)
        summed = summed + lax.optimization_barrier(partial_value.astype(jnp.bfloat16)).astype(jnp.float32)
    mixed = (tokens_wide + 0.5 * summed).astype(jnp.bfloat16)
    return (mixed, gate_ready, up_ready, down_ready)
```

```python
import jax
import jax.numpy as jnp
from jax import lax
from jax.sharding import Mesh
from jax.sharding import PartitionSpec as P

TP = ("z", "c")
ROWS = ("fs", "z", "c")


def move(array, by):
    planes = lax.axis_size("z")
    return lax.ppermute(array, "z", [(i, (i + by) % planes) for i in range(planes)])


def partial_sums(rows, weights):
    wide = rows.astype(jnp.float32)
    row_scale = lax.rsqrt(jnp.mean(wide * wide, axis=1, keepdims=True) + 1e-06)
    total = None
    for gate, up, down in weights:
        gate_proj = row_scale * jnp.dot(rows, gate, preferred_element_type=jnp.float32)
        up_proj = row_scale * jnp.dot(rows, up, preferred_element_type=jnp.float32)
        hidden = (jax.nn.silu(gate_proj) * up_proj).astype(jnp.bfloat16)
        share = lax.dot_general(hidden, down, (((1,), (1,)), ((), ())), preferred_element_type=jnp.float32)
        total = share if total is None else total + share
    return total


def unpacked(packed):
    return tuple(packed[:, k].reshape(-1, packed.shape[-1]) for k in range(3))


def body(tokens, norm_gain, gate_master, up_master, down_master):
    rows = tokens.shape[0]
    gain = norm_gain[:, None]
    shard = jnp.stack([(gain * gate_master).astype(jnp.bfloat16), (gain * up_master).astype(jnp.bfloat16), down_master.astype(jnp.bfloat16)])
    copies = jnp.broadcast_to(shard, (lax.axis_size("fs"), *shard.shape))
    packed = lax.all_to_all(copies, "fs", split_axis=0, concat_axis=0, tiled=True)

    far = move(tokens, 8)
    above = move(tokens, -4)
    below = move(tokens, 4)
    next_a = move(jnp.concatenate([tokens, far]), -1)
    prev_a = move(jnp.concatenate([tokens, far]), 1)
    next_b = move(jnp.concatenate([above, below]), -1)
    prev_b = move(jnp.concatenate([above, below]), 1)
    next2 = move(jnp.concatenate([tokens, above]), -2)
    prev2 = move(jnp.concatenate([tokens, below]), 2)

    partner = lax.ppermute(packed, "c", [(0, 1), (1, 0)])
    own_weights = unpacked(packed)
    weights = (own_weights, unpacked(partner))

    own = partial_sums(jnp.concatenate([tokens, far, above, below]), weights)
    ones = partial_sums(jnp.concatenate([next_a, next_b, prev_a, prev_b]), weights).astype(jnp.bfloat16)
    to_next = move(ones[: 4 * rows], 1)
    to_prev = move(ones[4 * rows :], -1)
    twos = partial_sums(jnp.concatenate([next2, prev2]), weights).astype(jnp.bfloat16)
    to_next2 = move(twos[: 2 * rows], 2)
    to_prev2 = move(twos[2 * rows :], -2)

    def block(array, k):
        return array[k * rows : (k + 1) * rows].astype(jnp.float32)

    sum_far = block(own, 1) + block(to_next, 1) + block(to_prev, 1)
    back_far = move(sum_far.astype(jnp.bfloat16), 8)
    sum_above = block(own, 2) + block(to_next, 2) + block(to_prev, 2) + block(to_next2, 1)
    back_above = move(sum_above.astype(jnp.bfloat16), 4)
    sum_below = block(own, 3) + block(to_next, 3) + block(to_prev, 3) + block(to_prev2, 1)
    back_below = move(sum_below.astype(jnp.bfloat16), -4)
    here = block(own, 0) + block(to_next, 0) + block(to_prev, 0) + block(to_next2, 0) + block(to_prev2, 0)
    summed = here + back_far.astype(jnp.float32) + back_above.astype(jnp.float32) + back_below.astype(jnp.float32)
    mixed = (tokens.astype(jnp.float32) + 0.5 * summed).astype(jnp.bfloat16)
    return (mixed, *own_weights)


def solution(mesh):
    split = Mesh(mesh.devices.reshape(mesh.shape["fs"], 16, 2), ROWS)
    placed = (P(ROWS, None), P("fs"), P("fs", TP), P("fs", TP), P("fs", TP))
    return jax.shard_map(
        body,
        mesh=split,
        in_specs=placed,
        out_specs=(P(ROWS, None), P(None, TP), P(None, TP), P(None, TP)),
        check_vma=False,
    )
```

```python
import jax
import jax.numpy as jnp
from jax import lax
from jax.experimental import pallas as pl
from jax.experimental.pallas import tpu as pltpu
from jax.sharding import Mesh
from jax.sharding import PartitionSpec as P


TP = ("z", "c")
ROWS = ("fs", "z", "c")
VMEM = pl.BlockSpec(memory_space=pltpu.VMEM)


def move(array, by):
    planes = lax.axis_size("z")
    return lax.ppermute(array, "z", [(i, (i + by) % planes) for i in range(planes)])


def sums_kernel(rows_ref, own_ref, partner_ref, out_ref):
    rows = rows_ref[...]
    width = rows.shape[1]
    wide = rows.astype(jnp.float32)
    row_scale = lax.rsqrt(jnp.mean(wide * wide, axis=1, keepdims=True) + 1e-06)
    hidden = []
    for ref in (own_ref, partner_ref):
        gate = ref[:, 0].reshape(width, -1)
        up = ref[:, 1].reshape(width, -1)
        gate_proj = row_scale * jnp.dot(rows, gate, preferred_element_type=jnp.float32)
        up_proj = row_scale * jnp.dot(rows, up, preferred_element_type=jnp.float32)
        hidden.append((gate_proj / (1.0 + jnp.exp(-gate_proj)) * up_proj).astype(jnp.bfloat16))
    total = None
    for ref, part in zip((own_ref, partner_ref), hidden):
        down = ref[:, 2].reshape(width, -1)
        share = lax.dot_general(part, down, (((1,), (1,)), ((), ())), preferred_element_type=jnp.float32)
        total = share if total is None else total + share
    out_ref[...] = total.astype(out_ref.dtype)


def partial_sums(rows, own, partner, dtype):
    units = 2 * own.shape[-1]
    count, width = rows.shape
    return pl.pallas_call(
        sums_kernel,
        out_shape=jax.ShapeDtypeStruct((count, width), dtype),
        in_specs=[VMEM, VMEM, VMEM],
        out_specs=VMEM,
        compiler_params=pltpu.CompilerParams(vmem_limit_bytes=32 * 1024 * 1024),
        cost_estimate=pl.CostEstimate(flops=6 * count * width * units, bytes_accessed=6 * width * units, transcendentals=count * units),
        name="sums",
    )(rows, own, partner)


def step(tokens, norm_gain, gate_master, up_master, down_master):
    rows = tokens.shape[0]
    gain = norm_gain[:, None]
    shard = jnp.stack([(gain * gate_master).astype(jnp.bfloat16), (gain * up_master).astype(jnp.bfloat16), down_master.astype(jnp.bfloat16)])
    copies = jnp.broadcast_to(shard, (lax.axis_size("fs"), *shard.shape))
    packed = lax.all_to_all(copies, "fs", split_axis=0, concat_axis=0, tiled=True)

    far = move(tokens, 8)
    above = move(tokens, -4)
    below = move(tokens, 4)
    held = jnp.concatenate([tokens, far, above, below])
    from_next = move(held, -1)
    from_prev = move(held, 1)
    from_next2 = move(jnp.concatenate([tokens, above]), -2)
    from_prev2 = move(jnp.concatenate([tokens, below]), 2)

    partner = lax.ppermute(packed, "c", [(0, 1), (1, 0)])

    ones = partial_sums(jnp.concatenate([from_next, from_prev]), packed, partner, jnp.bfloat16)
    to_next = move(ones[: 4 * rows], 1)
    to_prev = move(ones[4 * rows :], -1)
    twos = partial_sums(jnp.concatenate([from_next2, from_prev2]), packed, partner, jnp.bfloat16)
    to_next2 = move(twos[: 2 * rows], 2)
    to_prev2 = move(twos[2 * rows :], -2)
    own = partial_sums(held, packed, partner, jnp.float32)

    def block(array, k):
        return array[k * rows : (k + 1) * rows].astype(jnp.float32)

    sum_far = block(own, 1) + block(to_next, 1) + block(to_prev, 1)
    back_far = move(sum_far.astype(jnp.bfloat16), 8)
    sum_above = block(own, 2) + block(to_next, 2) + block(to_prev, 2) + block(to_next2, 1)
    back_above = move(sum_above.astype(jnp.bfloat16), 4)
    sum_below = block(own, 3) + block(to_next, 3) + block(to_prev, 3) + block(to_prev2, 1)
    back_below = move(sum_below.astype(jnp.bfloat16), -4)
    here = block(own, 0) + block(to_next, 0) + block(to_prev, 0) + block(to_next2, 0) + block(to_prev2, 0)
    summed = here + back_far.astype(jnp.float32) + back_above.astype(jnp.float32) + back_below.astype(jnp.float32)
    mixed = (tokens.astype(jnp.float32) + 0.5 * summed).astype(jnp.bfloat16)
    return (mixed, *(packed[:, k].reshape(-1, packed.shape[-1]) for k in range(3)))


def solution(mesh):
    split = Mesh(mesh.devices.reshape(mesh.shape["fs"], 16, 2), ROWS)
    placed = (P(ROWS, None), P("fs"), P("fs", TP), P("fs", TP), P("fs", TP))
    return jax.shard_map(
        step,
        mesh=split,
        in_specs=placed,
        out_specs=(P(ROWS, None), P(None, TP), P(None, TP), P(None, TP)),
        check_vma=False,
    )
```

```python
import jax
import jax.numpy as jnp
from jax import lax
from jax.experimental import pallas as pl
from jax.experimental.pallas import tpu as pltpu
from jax.sharding import Mesh
from jax.sharding import PartitionSpec as P


TP = ("z", "c")
ROWS = ("fs", "z", "c")
VMEM = pl.BlockSpec(memory_space=pltpu.VMEM)
PARAMS = pltpu.CompilerParams(vmem_limit_bytes=32 * 1024 * 1024)


def local(kernel, outs, *args, flops=0, transcendentals=0):
    moved = sum(a.size * a.dtype.itemsize for a in (*args, *outs))
    return pl.pallas_call(
        kernel,
        out_shape=outs,
        in_specs=[VMEM] * len(args),
        out_specs=tuple(VMEM for _ in outs),
        compiler_params=PARAMS,
        cost_estimate=pl.CostEstimate(flops=flops, bytes_accessed=moved, transcendentals=transcendentals),
    )(*args)


def move(array, by):
    planes = lax.axis_size("z")
    return lax.ppermute(array, "z", [(i, (i + by) % planes) for i in range(planes)])


def copies_kernel(gain_hbm, gate_hbm, up_hbm, down_hbm, out_hbm, gain_ref, wide_ref, shard_ref, in_sems, out_sems):
    loads = [pltpu.make_async_copy(gain_hbm, gain_ref, in_sems.at[3])]
    for k, source in enumerate((gate_hbm, up_hbm, down_hbm)):
        loads.append(pltpu.make_async_copy(source, wide_ref.at[k], in_sems.at[k]))
    for load in loads:
        load.start()
    loads[0].wait()
    count = gate_hbm.shape[0]
    gain = jnp.transpose(jnp.broadcast_to(gain_ref[...], (count, count)))
    gain = jnp.concatenate([gain] * (gate_hbm.shape[1] // count), axis=1)
    stores = []
    for k in range(3):
        loads[1 + k].wait()
        value = wide_ref[k]
        shard_ref[k] = (value if k == 2 else gain * value).astype(jnp.bfloat16)
    for i in range(out_hbm.shape[0]):
        stores.append(pltpu.make_async_copy(shard_ref, out_hbm.at[i], out_sems.at[i]))
        stores[-1].start()
    for store in stores:
        store.wait()


def weight_copies(norm_gain, gate_master, up_master, down_master, count):
    shape = (3, *gate_master.shape)
    anywhere = pl.BlockSpec(memory_space=pltpu.HBM)
    return pl.pallas_call(
        copies_kernel,
        out_shape=jax.ShapeDtypeStruct((count, *shape), jnp.bfloat16),
        in_specs=[anywhere] * 4,
        out_specs=anywhere,
        scratch_shapes=[
            pltpu.VMEM((1, norm_gain.shape[0]), jnp.float32),
            pltpu.VMEM(shape, jnp.float32),
            pltpu.VMEM(shape, jnp.bfloat16),
            pltpu.SemaphoreType.DMA((4,)),
            pltpu.SemaphoreType.DMA((count,)),
        ],
        compiler_params=pltpu.CompilerParams(vmem_limit_bytes=66846720),
        cost_estimate=pl.CostEstimate(flops=1000000, bytes_accessed=4000000, transcendentals=0),
        name="prepare",
    )(norm_gain.reshape(1, -1), gate_master, up_master, down_master)


def pack_kernel(*refs):
    *parts, out_ref = refs
    at = 0
    for ref in parts:
        out_ref[at : at + ref.shape[0]] = ref[...]
        at += ref.shape[0]


def pack(*parts):
    count = sum(p.shape[0] for p in parts)
    return local(pack_kernel, (jax.ShapeDtypeStruct((count, parts[0].shape[1]), parts[0].dtype),), *parts)[0]


def sums_kernel(count, *refs):
    rows_refs, (own_ref, partner_ref), out_refs = refs[:count], refs[count : count + 2], refs[count + 2 :]
    rows = jnp.concatenate([ref[...] for ref in rows_refs], axis=0)
    width = rows.shape[1]
    wide = rows.astype(jnp.float32)
    row_scale = lax.rsqrt(jnp.mean(wide * wide, axis=1, keepdims=True) + 1e-06)
    hidden = []
    for ref in (own_ref, partner_ref):
        gate = ref[:, 0].reshape(width, -1)
        up = ref[:, 1].reshape(width, -1)
        gate_proj = row_scale * jnp.dot(rows, gate, preferred_element_type=jnp.float32)
        up_proj = row_scale * jnp.dot(rows, up, preferred_element_type=jnp.float32)
        hidden.append((gate_proj / (1.0 + jnp.exp(-gate_proj)) * up_proj).astype(jnp.bfloat16))
    total = None
    for ref, part in zip((own_ref, partner_ref), hidden):
        down = ref[:, 2].reshape(width, -1)
        share = lax.dot_general(part, down, (((1,), (1,)), ((), ())), preferred_element_type=jnp.float32)
        total = share if total is None else total + share
    at = 0
    for ref in out_refs:
        ref[...] = total[at : at + ref.shape[0]].astype(ref.dtype)
        at += ref.shape[0]


def partial_sums(parts, weights, outs, dtype):
    units = 2 * weights[0].shape[-1]
    count, width = sum(p.shape[0] for p in parts), parts[0].shape[1]
    return local(
        lambda *refs: sums_kernel(len(parts), *refs),
        tuple(jax.ShapeDtypeStruct((count // outs, width), dtype) for _ in range(outs)),
        *parts,
        *weights,
        flops=6 * count * width * units,
        transcendentals=count * units,
    )


def fold_kernel(terms, *refs):
    inputs, outputs = refs[: len(refs) - len(terms)], refs[len(refs) - len(terms) :]
    for out_ref, pairs in zip(outputs, terms):
        rows = out_ref.shape[0]
        total = None
        for which, k in pairs:
            value = inputs[which][k * rows : (k + 1) * rows].astype(jnp.float32)
            total = value if total is None else total + value
        out_ref[...] = total.astype(out_ref.dtype)


def mix_kernel(tokens_ref, own_ref, next_ref, prev_ref, next2_ref, prev2_ref, far_ref, above_ref, below_ref, out_ref):
    rows = tokens_ref.shape[0]
    total = own_ref[:rows]
    for ref in (next_ref, prev_ref, next2_ref, prev2_ref, far_ref, above_ref, below_ref):
        total = total + ref[:rows].astype(jnp.float32)
    out_ref[...] = (tokens_ref[...].astype(jnp.float32) + 0.5 * total).astype(out_ref.dtype)


def step(tokens, norm_gain, gate_master, up_master, down_master):
    far = move(tokens, 8)
    copies = weight_copies(norm_gain, gate_master, up_master, down_master, lax.axis_size("fs"))
    packed = lax.all_to_all(copies, "fs", split_axis=0, concat_axis=0, tiled=True)
    above = move(tokens, -4)
    below = move(tokens, 4)
    held = pack(tokens, far, above, below)
    from_next = move(held, -1)
    from_prev = move(held, 1)
    from_next2 = move(pack(tokens, above), -2)
    from_prev2 = move(pack(tokens, below), 2)

    partner = lax.ppermute(packed, "c", [(0, 1), (1, 0)])
    weights = (packed, partner)

    ones_next, ones_prev = partial_sums((from_next, from_prev), weights, 2, jnp.bfloat16)
    to_next = move(ones_next, 1)
    to_prev = move(ones_prev, -1)
    twos_next, twos_prev = partial_sums((from_next2, from_prev2), weights, 2, jnp.bfloat16)
    to_next2 = move(twos_next, 2)
    to_prev2 = move(twos_prev, -2)
    (own,) = partial_sums((held,), weights, 1, jnp.float32)

    block = jax.ShapeDtypeStruct(tokens.shape, jnp.bfloat16)
    (sum_far,) = local(lambda *refs: fold_kernel((((0, 1), (1, 1), (2, 1)),), *refs), (block,), own, to_next, to_prev)
    back_far = move(sum_far, 8)
    terms = (((0, 2), (1, 2), (2, 2), (3, 1)), ((0, 3), (1, 3), (2, 3), (4, 1)))
    sum_above, sum_below = local(lambda *refs: fold_kernel(terms, *refs), (block, block), own, to_next, to_prev, to_next2, to_prev2)
    back_above = move(sum_above, 4)
    back_below = move(sum_below, -4)
    (mixed,) = local(mix_kernel, (block,), tokens, own, to_next, to_prev, to_next2, to_prev2, back_far, back_above, back_below)
    return (mixed, *(packed[:, k].reshape(-1, packed.shape[-1]) for k in range(3)))


def solution(mesh):
    split = Mesh(mesh.devices.reshape(mesh.shape["fs"], 16, 2), ROWS)
    placed = (P(ROWS, None), P("fs"), P("fs", TP), P("fs", TP), P("fs", TP))
    return jax.shard_map(
        step,
        mesh=split,
        in_specs=placed,
        out_specs=(P(ROWS, None), P(None, TP), P(None, TP), P(None, TP)),
        check_vma=False,
    )
```

```python
import jax
import jax.numpy as jnp
from jax import lax
from jax.experimental import pallas as pl
from jax.experimental.pallas import tpu as pltpu
from jax.sharding import Mesh
from jax.sharding import PartitionSpec as P


TP = ("z", "c")
ROWS = ("fs", "z", "c")
VMEM = pl.BlockSpec(memory_space=pltpu.VMEM)
PARAMS = pltpu.CompilerParams(vmem_limit_bytes=32 * 1024 * 1024)


def local(kernel, outs, *args, flops=0, transcendentals=0):
    moved = sum(a.size * a.dtype.itemsize for a in (*args, *outs))
    return pl.pallas_call(
        kernel,
        out_shape=outs,
        in_specs=[VMEM] * len(args),
        out_specs=tuple(VMEM for _ in outs),
        compiler_params=PARAMS,
        cost_estimate=pl.CostEstimate(flops=flops, bytes_accessed=moved, transcendentals=transcendentals),
    )(*args)


def move(array, by):
    planes = lax.axis_size("z")
    return lax.ppermute(array, "z", [(i, (i + by) % planes) for i in range(planes)])


def copies_kernel(gain_hbm, gate_hbm, up_hbm, down_hbm, out_hbm, gain_ref, wide_ref, shard_ref, in_sems, out_sems):
    loads = [pltpu.make_async_copy(gain_hbm, gain_ref, in_sems.at[3])]
    for k, source in enumerate((gate_hbm, up_hbm, down_hbm)):
        loads.append(pltpu.make_async_copy(source, wide_ref.at[k], in_sems.at[k]))
    for load in loads:
        load.start()
    loads[0].wait()
    count = gate_hbm.shape[0]
    gain = jnp.transpose(jnp.broadcast_to(gain_ref[...], (count, count)))
    gain = jnp.concatenate([gain] * (gate_hbm.shape[1] // count), axis=1)
    stores = []
    for k in range(3):
        loads[1 + k].wait()
        value = wide_ref[k]
        shard_ref[k] = (value if k == 2 else gain * value).astype(jnp.bfloat16)
    for i in range(out_hbm.shape[0]):
        stores.append(pltpu.make_async_copy(shard_ref, out_hbm.at[i], out_sems.at[i]))
        stores[-1].start()
    for store in stores:
        store.wait()


def weight_copies(norm_gain, gate_master, up_master, down_master, count):
    shape = (3, *gate_master.shape)
    anywhere = pl.BlockSpec(memory_space=pltpu.HBM)
    return pl.pallas_call(
        copies_kernel,
        out_shape=jax.ShapeDtypeStruct((count, *shape), jnp.bfloat16),
        in_specs=[anywhere] * 4,
        out_specs=anywhere,
        scratch_shapes=[
            pltpu.VMEM((1, norm_gain.shape[0]), jnp.float32),
            pltpu.VMEM(shape, jnp.float32),
            pltpu.VMEM(shape, jnp.bfloat16),
            pltpu.SemaphoreType.DMA((4,)),
            pltpu.SemaphoreType.DMA((count,)),
        ],
        compiler_params=pltpu.CompilerParams(vmem_limit_bytes=66846720),
        cost_estimate=pl.CostEstimate(flops=1000000, bytes_accessed=4000000, transcendentals=0),
        name="prepare",
    )(norm_gain.reshape(1, -1), gate_master, up_master, down_master)


def pack_kernel(*refs):
    *parts, out_ref = refs
    at = 0
    for ref in parts:
        out_ref[at : at + ref.shape[0]] = ref[...]
        at += ref.shape[0]


def pack_pairs_kernel(first_ref, *refs):
    parts, out_refs = refs[: len(refs) // 2], refs[len(refs) // 2 :]
    for ref, out_ref in zip(parts, out_refs):
        pack_kernel(first_ref, ref, out_ref)


def pack(*parts):
    count = sum(p.shape[0] for p in parts)
    return local(pack_kernel, (jax.ShapeDtypeStruct((count, parts[0].shape[1]), parts[0].dtype),), *parts)[0]


def sums_kernel(count, *refs):
    rows_refs, (own_ref, partner_ref), out_refs = refs[:count], refs[count : count + 2], refs[count + 2 :]
    rows = jnp.concatenate([ref[...] for ref in rows_refs], axis=0)
    width = rows.shape[1]
    wide = rows.astype(jnp.float32)
    row_scale = lax.rsqrt(jnp.mean(wide * wide, axis=1, keepdims=True) + 1e-06)
    hidden = []
    for ref in (own_ref, partner_ref):
        gate = ref[:, 0].reshape(width, -1)
        up = ref[:, 1].reshape(width, -1)
        gate_proj = row_scale * jnp.dot(rows, gate, preferred_element_type=jnp.float32)
        up_proj = row_scale * jnp.dot(rows, up, preferred_element_type=jnp.float32)
        hidden.append((gate_proj / (1.0 + jnp.exp(-gate_proj)) * up_proj).astype(jnp.bfloat16))
    total = None
    for ref, part in zip((own_ref, partner_ref), hidden):
        down = ref[:, 2].reshape(width, -1)
        share = lax.dot_general(part, down, (((1,), (1,)), ((), ())), preferred_element_type=jnp.float32)
        total = share if total is None else total + share
    at = 0
    for ref in out_refs:
        ref[...] = total[at : at + ref.shape[0]].astype(ref.dtype)
        at += ref.shape[0]


def partial_sums(parts, weights, outs, dtype):
    units = 2 * weights[0].shape[-1]
    count, width = sum(p.shape[0] for p in parts), parts[0].shape[1]
    return local(
        lambda *refs: sums_kernel(len(parts), *refs),
        tuple(jax.ShapeDtypeStruct((count // outs, width), dtype) for _ in range(outs)),
        *parts,
        *weights,
        flops=6 * count * width * units,
        transcendentals=count * units,
    )


def fold_kernel(terms, *refs):
    inputs, outputs = refs[: len(refs) - len(terms)], refs[len(refs) - len(terms) :]
    for out_ref, pairs in zip(outputs, terms):
        rows = out_ref.shape[0]
        total = None
        for which, k in pairs:
            value = inputs[which][k * rows : (k + 1) * rows].astype(jnp.float32)
            total = value if total is None else total + value
        out_ref[...] = total.astype(out_ref.dtype)


def mix_kernel(tokens_ref, own_ref, next_ref, prev_ref, next2_ref, prev2_ref, far_ref, above_ref, below_ref, out_ref):
    rows = tokens_ref.shape[0]
    total = own_ref[:rows]
    for ref in (next_ref, prev_ref, next2_ref, prev2_ref, far_ref, above_ref, below_ref):
        total = total + ref[:rows].astype(jnp.float32)
    out_ref[...] = (tokens_ref[...].astype(jnp.float32) + 0.5 * total).astype(out_ref.dtype)


def step(tokens, norm_gain, gate_master, up_master, down_master):
    copies = weight_copies(norm_gain, gate_master, up_master, down_master, lax.axis_size("fs"))
    packed = lax.all_to_all(copies, "fs", split_axis=0, concat_axis=0, tiled=True)
    above = move(tokens, -4)
    below = move(tokens, 4)
    far = move(tokens, 8)
    pair = jax.ShapeDtypeStruct((2 * tokens.shape[0], tokens.shape[1]), tokens.dtype)
    pair_above, pair_below = local(pack_pairs_kernel, (pair, pair), tokens, above, below)
    from_next2 = move(pair_above, -2)
    from_prev2 = move(pair_below, 2)
    held = pack(tokens, far, above, below)
    from_next = move(held, -1)
    from_prev = move(held, 1)

    partner = lax.ppermute(packed, "c", [(0, 1), (1, 0)])
    weights = (packed, partner)

    ones_next, ones_prev = partial_sums((from_next, from_prev), weights, 2, jnp.bfloat16)
    to_next = move(ones_next, 1)
    to_prev = move(ones_prev, -1)
    twos_next, twos_prev = partial_sums((from_next2, from_prev2), weights, 2, jnp.bfloat16)
    to_next2 = move(twos_next, 2)
    to_prev2 = move(twos_prev, -2)
    (own,) = partial_sums((held,), weights, 1, jnp.float32)

    block = jax.ShapeDtypeStruct(tokens.shape, jnp.bfloat16)
    (sum_far,) = local(lambda *refs: fold_kernel((((0, 1), (1, 1), (2, 1)),), *refs), (block,), own, to_next, to_prev)
    back_far = move(sum_far, 8)
    terms = (((0, 2), (1, 2), (2, 2), (3, 1)), ((0, 3), (1, 3), (2, 3), (4, 1)))
    sum_above, sum_below = local(lambda *refs: fold_kernel(terms, *refs), (block, block), own, to_next, to_prev, to_next2, to_prev2)
    back_above = move(sum_above, 4)
    back_below = move(sum_below, -4)
    (mixed,) = local(mix_kernel, (block,), tokens, own, to_next, to_prev, to_next2, to_prev2, back_far, back_above, back_below)
    return (mixed, *(packed[:, k].reshape(-1, packed.shape[-1]) for k in range(3)))


def solution(mesh):
    split = Mesh(mesh.devices.reshape(mesh.shape["fs"], 16, 2), ROWS)
    placed = (P(ROWS, None), P("fs"), P("fs", TP), P("fs", TP), P("fs", TP))
    return jax.shard_map(
        step,
        mesh=split,
        in_specs=placed,
        out_specs=(P(ROWS, None), P(None, TP), P(None, TP), P(None, TP)),
        check_vma=False,
    )
```

```python
import jax
import jax.numpy as jnp
from jax import lax
from jax.experimental import pallas as pl
from jax.experimental.pallas import tpu as pltpu
from jax.sharding import Mesh
from jax.sharding import PartitionSpec as P


TP = ("z", "c")
ROWS = ("fs", "z", "c")
VMEM = pl.BlockSpec(memory_space=pltpu.VMEM)
PARAMS = pltpu.CompilerParams(vmem_limit_bytes=32 * 1024 * 1024)


def local(kernel, outs, *args, flops=0, transcendentals=0):
    moved = sum(a.size * a.dtype.itemsize for a in (*args, *outs))
    return pl.pallas_call(
        kernel,
        out_shape=outs,
        in_specs=[VMEM] * len(args),
        out_specs=tuple(VMEM for _ in outs),
        compiler_params=PARAMS,
        cost_estimate=pl.CostEstimate(flops=flops, bytes_accessed=moved, transcendentals=transcendentals),
    )(*args)


def move(array, by):
    planes = lax.axis_size("z")
    return lax.ppermute(array, "z", [(i, (i + by) % planes) for i in range(planes)])


def copies_kernel(gain_hbm, gate_hbm, up_hbm, down_hbm, out_hbm, gain_ref, wide_ref, shard_ref, in_sems, out_sems):
    loads = [pltpu.make_async_copy(gain_hbm, gain_ref, in_sems.at[3])]
    for k, source in enumerate((gate_hbm, up_hbm, down_hbm)):
        loads.append(pltpu.make_async_copy(source, wide_ref.at[k], in_sems.at[k]))
    for load in loads:
        load.start()
    loads[0].wait()
    count = gate_hbm.shape[0]
    gain = jnp.transpose(jnp.broadcast_to(gain_ref[...], (count, count)))
    gain = jnp.concatenate([gain] * (gate_hbm.shape[1] // count), axis=1)
    stores = []
    for k in range(3):
        loads[1 + k].wait()
        value = wide_ref[k]
        shard_ref[k] = (value if k == 2 else gain * value).astype(jnp.bfloat16)
    for i in range(out_hbm.shape[0]):
        stores.append(pltpu.make_async_copy(shard_ref, out_hbm.at[i], out_sems.at[i]))
        stores[-1].start()
    for store in stores:
        store.wait()


def weight_copies(norm_gain, gate_master, up_master, down_master, count):
    shape = (3, *gate_master.shape)
    anywhere = pl.BlockSpec(memory_space=pltpu.HBM)
    return pl.pallas_call(
        copies_kernel,
        out_shape=jax.ShapeDtypeStruct((count, *shape), jnp.bfloat16),
        in_specs=[anywhere] * 4,
        out_specs=anywhere,
        scratch_shapes=[
            pltpu.VMEM((1, norm_gain.shape[0]), jnp.float32),
            pltpu.VMEM(shape, jnp.float32),
            pltpu.VMEM(shape, jnp.bfloat16),
            pltpu.SemaphoreType.DMA((4,)),
            pltpu.SemaphoreType.DMA((count,)),
        ],
        compiler_params=pltpu.CompilerParams(vmem_limit_bytes=66846720),
        cost_estimate=pl.CostEstimate(flops=1000000, bytes_accessed=4000000, transcendentals=0),
        name="prepare",
    )(norm_gain.reshape(1, -1), gate_master, up_master, down_master)


def pack_kernel(*refs):
    *parts, out_ref = refs
    at = 0
    for ref in parts:
        out_ref[at : at + ref.shape[0]] = ref[...]
        at += ref.shape[0]


def pack(*parts):
    count = sum(p.shape[0] for p in parts)
    return local(pack_kernel, (jax.ShapeDtypeStruct((count, parts[0].shape[1]), parts[0].dtype),), *parts)[0]


def sums_kernel(count, *refs):
    rows_refs, (own_ref, partner_ref), out_refs = refs[:count], refs[count : count + 2], refs[count + 2 :]
    rows = jnp.concatenate([ref[...] for ref in rows_refs], axis=0)
    width = rows.shape[1]
    wide = rows.astype(jnp.float32)
    row_scale = lax.rsqrt(jnp.mean(wide * wide, axis=1, keepdims=True) + 1e-06)
    hidden = []
    for ref in (own_ref, partner_ref):
        gate = ref[:, 0].reshape(width, -1)
        up = ref[:, 1].reshape(width, -1)
        gate_proj = row_scale * jnp.dot(rows, gate, preferred_element_type=jnp.float32)
        up_proj = row_scale * jnp.dot(rows, up, preferred_element_type=jnp.float32)
        hidden.append((gate_proj / (1.0 + jnp.exp(-gate_proj)) * up_proj).astype(jnp.bfloat16))
    total = None
    for ref, part in zip((own_ref, partner_ref), hidden):
        down = ref[:, 2].reshape(width, -1)
        share = lax.dot_general(part, down, (((1,), (1,)), ((), ())), preferred_element_type=jnp.float32)
        total = share if total is None else total + share
    at = 0
    for ref in out_refs:
        ref[...] = total[at : at + ref.shape[0]].astype(ref.dtype)
        at += ref.shape[0]


def partial_sums(parts, weights, outs, dtype):
    units = 2 * weights[0].shape[-1]
    count, width = sum(p.shape[0] for p in parts), parts[0].shape[1]
    return local(
        lambda *refs: sums_kernel(len(parts), *refs),
        tuple(jax.ShapeDtypeStruct((count // outs, width), dtype) for _ in range(outs)),
        *parts,
        *weights,
        flops=6 * count * width * units,
        transcendentals=count * units,
    )


def fold_kernel(terms, *refs):
    inputs, outputs = refs[: len(refs) - len(terms)], refs[len(refs) - len(terms) :]
    for out_ref, pairs in zip(outputs, terms):
        rows = out_ref.shape[0]
        total = None
        for which, k in pairs:
            value = inputs[which][k * rows : (k + 1) * rows].astype(jnp.float32)
            total = value if total is None else total + value
        out_ref[...] = total.astype(out_ref.dtype)


def mix_kernel(tokens_ref, own_ref, next_ref, prev_ref, next2_ref, prev2_ref, far_ref, above_ref, below_ref, out_ref):
    rows = tokens_ref.shape[0]
    total = own_ref[:rows]
    for ref in (next_ref, prev_ref, next2_ref, prev2_ref, far_ref, above_ref, below_ref):
        total = total + ref[:rows].astype(jnp.float32)
    out_ref[...] = (tokens_ref[...].astype(jnp.float32) + 0.5 * total).astype(out_ref.dtype)


def step(tokens, norm_gain, gate_master, up_master, down_master):
    copies = weight_copies(norm_gain, gate_master, up_master, down_master, lax.axis_size("fs"))
    packed = lax.all_to_all(copies, "fs", split_axis=0, concat_axis=0, tiled=True)
    far = move(tokens, 8)
    above = move(tokens, -4)
    below = move(tokens, 4)
    own_next2 = move(tokens, -2)
    own_prev2 = move(tokens, 2)
    held = pack(tokens, far, above, below)
    from_next = move(held, -1)
    from_prev = move(held, 1)
    from_next2 = (own_next2, move(above, -2))
    from_prev2 = (own_prev2, move(below, 2))

    partner = lax.ppermute(packed, "c", [(0, 1), (1, 0)])
    weights = (packed, partner)

    ones_next, ones_prev = partial_sums((from_next, from_prev), weights, 2, jnp.bfloat16)
    to_next = move(ones_next, 1)
    to_prev = move(ones_prev, -1)
    twos_next, twos_prev = partial_sums((*from_next2, *from_prev2), weights, 2, jnp.bfloat16)
    to_next2 = move(twos_next, 2)
    to_prev2 = move(twos_prev, -2)
    (own,) = partial_sums((held,), weights, 1, jnp.float32)

    block = jax.ShapeDtypeStruct(tokens.shape, jnp.bfloat16)
    (sum_far,) = local(lambda *refs: fold_kernel((((0, 1), (1, 1), (2, 1)),), *refs), (block,), own, to_next, to_prev)
    back_far = move(sum_far, 8)
    terms = (((0, 2), (1, 2), (2, 2), (3, 1)), ((0, 3), (1, 3), (2, 3), (4, 1)))
    sum_above, sum_below = local(lambda *refs: fold_kernel(terms, *refs), (block, block), own, to_next, to_prev, to_next2, to_prev2)
    back_above = move(sum_above, 4)
    back_below = move(sum_below, -4)
    (mixed,) = local(mix_kernel, (block,), tokens, own, to_next, to_prev, to_next2, to_prev2, back_far, back_above, back_below)
    return (mixed, *(packed[:, k].reshape(-1, packed.shape[-1]) for k in range(3)))


def solution(mesh):
    split = Mesh(mesh.devices.reshape(mesh.shape["fs"], 16, 2), ROWS)
    placed = (P(ROWS, None), P("fs"), P("fs", TP), P("fs", TP), P("fs", TP))
    return jax.shard_map(
        step,
        mesh=split,
        in_specs=placed,
        out_specs=(P(ROWS, None), P(None, TP), P(None, TP), P(None, TP)),
        check_vma=False,
    )
```

```python
import jax
import jax.numpy as jnp
from jax import lax
from jax.experimental import pallas as pl
from jax.experimental.pallas import tpu as pltpu
from jax.sharding import Mesh
from jax.sharding import PartitionSpec as P


Z = ("zh", "zl")
TP = (*Z, "c")
ROWS = ("fs", *TP)
VMEM = pl.BlockSpec(memory_space=pltpu.VMEM)
PARAMS = pltpu.CompilerParams(vmem_limit_bytes=32 * 1024 * 1024)


def local(kernel, outs, *args, flops=0, transcendentals=0):
    moved = sum(a.size * a.dtype.itemsize for a in (*args, *outs))
    return pl.pallas_call(
        kernel,
        out_shape=outs,
        in_specs=[VMEM] * len(args),
        out_specs=tuple(VMEM for _ in outs),
        compiler_params=PARAMS,
        cost_estimate=pl.CostEstimate(flops=flops, bytes_accessed=moved, transcendentals=transcendentals),
    )(*args)


def move(array, by):
    planes = lax.axis_size(Z)
    return lax.ppermute(array, Z, [(i, (i + by) % planes) for i in range(planes)])


def copies_kernel(gain_hbm, gate_hbm, up_hbm, down_hbm, out_hbm, gain_ref, wide_ref, shard_ref, in_sems, out_sems):
    loads = [pltpu.make_async_copy(gain_hbm, gain_ref, in_sems.at[3])]
    for k, source in enumerate((gate_hbm, up_hbm, down_hbm)):
        loads.append(pltpu.make_async_copy(source, wide_ref.at[k], in_sems.at[k]))
    for load in loads:
        load.start()
    loads[0].wait()
    count = gate_hbm.shape[0]
    gain = jnp.transpose(jnp.broadcast_to(gain_ref[...], (count, count)))
    gain = jnp.concatenate([gain] * (gate_hbm.shape[1] // count), axis=1)
    stores = []
    for k in range(3):
        loads[1 + k].wait()
        value = wide_ref[k]
        shard_ref[k] = (value if k == 2 else gain * value).astype(jnp.bfloat16)
    for i in range(out_hbm.shape[0]):
        stores.append(pltpu.make_async_copy(shard_ref, out_hbm.at[i], out_sems.at[i]))
        stores[-1].start()
    for store in stores:
        store.wait()


def weight_copies(norm_gain, gate_master, up_master, down_master, count):
    shape = (3, *gate_master.shape)
    anywhere = pl.BlockSpec(memory_space=pltpu.HBM)
    return pl.pallas_call(
        copies_kernel,
        out_shape=jax.ShapeDtypeStruct((count, *shape), jnp.bfloat16),
        in_specs=[anywhere] * 4,
        out_specs=anywhere,
        scratch_shapes=[
            pltpu.VMEM((1, norm_gain.shape[0]), jnp.float32),
            pltpu.VMEM(shape, jnp.float32),
            pltpu.VMEM(shape, jnp.bfloat16),
            pltpu.SemaphoreType.DMA((4,)),
            pltpu.SemaphoreType.DMA((count,)),
        ],
        compiler_params=pltpu.CompilerParams(vmem_limit_bytes=66846720),
        cost_estimate=pl.CostEstimate(flops=1000000, bytes_accessed=4000000, transcendentals=0),
        name="prepare",
    )(norm_gain.reshape(1, -1), gate_master, up_master, down_master)


def sums_kernel(count, *refs):
    rows_refs, (own_ref, partner_ref), out_refs = refs[:count], refs[count : count + 2], refs[count + 2 :]
    rows = jnp.concatenate([ref[...] for ref in rows_refs], axis=0)
    width = rows.shape[1]
    wide = rows.astype(jnp.float32)
    row_scale = lax.rsqrt(jnp.mean(wide * wide, axis=1, keepdims=True) + 1e-06)
    hidden = []
    for ref in (own_ref, partner_ref):
        gate = ref[:, 0].reshape(width, -1)
        up = ref[:, 1].reshape(width, -1)
        gate_proj = row_scale * jnp.dot(rows, gate, preferred_element_type=jnp.float32)
        up_proj = row_scale * jnp.dot(rows, up, preferred_element_type=jnp.float32)
        hidden.append((gate_proj / (1.0 + jnp.exp(-gate_proj)) * up_proj).astype(jnp.bfloat16))
    total = None
    for ref, part in zip((own_ref, partner_ref), hidden):
        down = ref[:, 2].reshape(width, -1)
        share = lax.dot_general(part, down, (((1,), (1,)), ((), ())), preferred_element_type=jnp.float32)
        total = share if total is None else total + share
    at = 0
    for ref in out_refs:
        ref[...] = total[at : at + ref.shape[0]].astype(ref.dtype)
        at += ref.shape[0]


def partial_sums(parts, weights, outs, dtype):
    units = 2 * weights[0].shape[-1]
    count, width = sum(p.shape[0] for p in parts), parts[0].shape[1]
    return local(
        lambda *refs: sums_kernel(len(parts), *refs),
        tuple(jax.ShapeDtypeStruct((count // outs, width), dtype) for _ in range(outs)),
        *parts,
        *weights,
        flops=6 * count * width * units,
        transcendentals=count * units,
    )


def fold_kernel(terms, *refs):
    inputs, outputs = refs[: len(refs) - len(terms)], refs[len(refs) - len(terms) :]
    for out_ref, pairs in zip(outputs, terms):
        rows = out_ref.shape[0]
        total = None
        for which, k in pairs:
            value = inputs[which][k * rows : (k + 1) * rows].astype(jnp.float32)
            total = value if total is None else total + value
        out_ref[...] = total.astype(out_ref.dtype)


def mix_kernel(tokens_ref, sums_ref, out_ref):
    total = sums_ref[0].astype(jnp.float32)
    for k in range(1, sums_ref.shape[0]):
        total = total + sums_ref[k].astype(jnp.float32)
    out_ref[...] = (tokens_ref[...].astype(jnp.float32) + 0.5 * total).astype(out_ref.dtype)


def fold_kernel(own_ref, next_ref, prev_ref, next2_ref, prev2_ref, out_ref):
    half = out_ref.shape[0] // 2
    for at, ref in ((0, next2_ref), (half, prev2_ref)):
        total = own_ref[at : at + half]
        for other in (next_ref, prev_ref):
            total = total + other[at : at + half].astype(jnp.float32)
        out_ref[at : at + half] = (total + ref[...].astype(jnp.float32)).astype(out_ref.dtype)


def step(tokens, norm_gain, gate_master, up_master, down_master):
    rows, width = tokens.shape
    groups = lax.axis_size("zh")
    copies = weight_copies(norm_gain, gate_master, up_master, down_master, lax.axis_size("fs"))
    packed = lax.all_to_all(copies, "fs", split_axis=0, concat_axis=0, tiled=True)
    held = lax.all_gather(tokens, "zh", axis=0, tiled=True)
    half = groups // 2 * rows
    from_next = move(held, -1)
    from_prev = move(held, 1)
    from_next2 = move(held[:half], -2)
    from_prev2 = move(held[half:], 2)

    partner = lax.ppermute(packed, "c", [(0, 1), (1, 0)])
    weights = (packed, partner)

    ones_next, ones_prev = partial_sums((from_next, from_prev), weights, 2, jnp.bfloat16)
    to_next = move(ones_next, 1)
    to_prev = move(ones_prev, -1)
    twos_next, twos_prev = partial_sums((from_next2, from_prev2), weights, 2, jnp.bfloat16)
    to_next2 = move(twos_next, 2)
    to_prev2 = move(twos_prev, -2)
    (own,) = partial_sums((held,), weights, 1, jnp.float32)

    (sums,) = local(fold_kernel, (jax.ShapeDtypeStruct((groups * rows, width), jnp.bfloat16),), own, to_next, to_prev, to_next2, to_prev2)
    sums = lax.all_to_all(sums.reshape(groups, rows, width), "zh", split_axis=0, concat_axis=0, tiled=True)
    (mixed,) = local(mix_kernel, (jax.ShapeDtypeStruct((rows, width), jnp.bfloat16),), tokens, sums)
    return (mixed, *(packed[:, k].reshape(-1, packed.shape[-1]) for k in range(3)))


def solution(mesh):
    split = Mesh(mesh.devices.reshape(mesh.shape["fs"], 4, 4, 2), ROWS)
    placed = (P(ROWS, None), P("fs"), P("fs", TP), P("fs", TP), P("fs", TP))
    return jax.shard_map(
        step,
        mesh=split,
        in_specs=placed,
        out_specs=(P(ROWS, None), P(None, TP), P(None, TP), P(None, TP)),
        check_vma=False,
    )
```

```python
import jax
import jax.numpy as jnp
from jax import lax
from jax.experimental import pallas as pl
from jax.experimental.pallas import tpu as pltpu
from jax.sharding import Mesh
from jax.sharding import PartitionSpec as P


Z = ("zh", "zl")
TP = (*Z, "c")
ROWS = ("fs", *TP)
VMEM = pl.BlockSpec(memory_space=pltpu.VMEM)
PARAMS = pltpu.CompilerParams(vmem_limit_bytes=32 * 1024 * 1024)


def local(kernel, outs, *args, flops=0, transcendentals=0):
    moved = sum(a.size * a.dtype.itemsize for a in (*args, *outs))
    return pl.pallas_call(
        kernel,
        out_shape=outs,
        in_specs=[VMEM] * len(args),
        out_specs=tuple(VMEM for _ in outs),
        compiler_params=PARAMS,
        cost_estimate=pl.CostEstimate(flops=flops, bytes_accessed=moved, transcendentals=transcendentals),
    )(*args)


def move(array, by):
    planes = lax.axis_size(Z)
    return lax.ppermute(array, Z, [(i, (i + by) % planes) for i in range(planes)])


def copies_kernel(gain_hbm, gate_hbm, up_hbm, down_hbm, out_hbm, gain_ref, wide_ref, shard_ref, in_sems, out_sems):
    loads = [pltpu.make_async_copy(gain_hbm, gain_ref, in_sems.at[3])]
    for k, source in enumerate((gate_hbm, up_hbm, down_hbm)):
        loads.append(pltpu.make_async_copy(source, wide_ref.at[k], in_sems.at[k]))
    for load in loads:
        load.start()
    loads[0].wait()
    count = gate_hbm.shape[0]
    gain = jnp.transpose(jnp.broadcast_to(gain_ref[...], (count, count)))
    gain = jnp.concatenate([gain] * (gate_hbm.shape[1] // count), axis=1)
    stores = []
    for k in range(3):
        loads[1 + k].wait()
        value = wide_ref[k]
        shard_ref[k] = (value if k == 2 else gain * value).astype(jnp.bfloat16)
    for i in range(out_hbm.shape[0]):
        stores.append(pltpu.make_async_copy(shard_ref, out_hbm.at[i], out_sems.at[i]))
        stores[-1].start()
    for store in stores:
        store.wait()


def weight_copies(norm_gain, gate_master, up_master, down_master, count):
    shape = (3, *gate_master.shape)
    anywhere = pl.BlockSpec(memory_space=pltpu.HBM)
    return pl.pallas_call(
        copies_kernel,
        out_shape=jax.ShapeDtypeStruct((count, *shape), jnp.bfloat16),
        in_specs=[anywhere] * 4,
        out_specs=anywhere,
        scratch_shapes=[
            pltpu.VMEM((1, norm_gain.shape[0]), jnp.float32),
            pltpu.VMEM(shape, jnp.float32),
            pltpu.VMEM(shape, jnp.bfloat16),
            pltpu.SemaphoreType.DMA((4,)),
            pltpu.SemaphoreType.DMA((count,)),
        ],
        compiler_params=pltpu.CompilerParams(vmem_limit_bytes=66846720),
        cost_estimate=pl.CostEstimate(flops=1000000, bytes_accessed=4000000, transcendentals=0),
        name="prepare",
    )(norm_gain.reshape(1, -1), gate_master, up_master, down_master)


def order_kernel(from_ref, held_ref, above_ref, below_ref):
    rows = from_ref.shape[0] // 4
    here = lax.axis_index("zh")

    def block(by):
        return from_ref[pl.ds(pl.multiple_of((here + by) % 4 * rows, rows), rows)]

    own, above, below = block(0), block(1), block(3)
    for k, value in enumerate((own, block(2), above, below)):
        held_ref[k * rows : (k + 1) * rows] = value
    for ref, value in ((above_ref, above), (below_ref, below)):
        ref[:rows] = own
        ref[rows:] = value


def sums_kernel(count, *refs):
    rows_refs, (own_ref, partner_ref), out_refs = refs[:count], refs[count : count + 2], refs[count + 2 :]
    rows = jnp.concatenate([ref[...] for ref in rows_refs], axis=0)
    width = rows.shape[1]
    wide = rows.astype(jnp.float32)
    row_scale = lax.rsqrt(jnp.mean(wide * wide, axis=1, keepdims=True) + 1e-06)
    hidden = []
    for ref in (own_ref, partner_ref):
        gate = ref[:, 0].reshape(width, -1)
        up = ref[:, 1].reshape(width, -1)
        gate_proj = row_scale * jnp.dot(rows, gate, preferred_element_type=jnp.float32)
        up_proj = row_scale * jnp.dot(rows, up, preferred_element_type=jnp.float32)
        hidden.append((gate_proj / (1.0 + jnp.exp(-gate_proj)) * up_proj).astype(jnp.bfloat16))
    total = None
    for ref, part in zip((own_ref, partner_ref), hidden):
        down = ref[:, 2].reshape(width, -1)
        share = lax.dot_general(part, down, (((1,), (1,)), ((), ())), preferred_element_type=jnp.float32)
        total = share if total is None else total + share
    at = 0
    for ref in out_refs:
        ref[...] = total[at : at + ref.shape[0]].astype(ref.dtype)
        at += ref.shape[0]


def partial_sums(parts, weights, outs, dtype):
    units = 2 * weights[0].shape[-1]
    count, width = sum(p.shape[0] for p in parts), parts[0].shape[1]
    return local(
        lambda *refs: sums_kernel(len(parts), *refs),
        tuple(jax.ShapeDtypeStruct((count // outs, width), dtype) for _ in range(outs)),
        *parts,
        *weights,
        flops=6 * count * width * units,
        transcendentals=count * units,
    )


def fold_kernel(terms, *refs):
    inputs, outputs = refs[: len(refs) - len(terms)], refs[len(refs) - len(terms) :]
    for out_ref, pairs in zip(outputs, terms):
        rows = out_ref.shape[0]
        total = None
        for which, k in pairs:
            value = inputs[which][k * rows : (k + 1) * rows].astype(jnp.float32)
            total = value if total is None else total + value
        out_ref[...] = total.astype(out_ref.dtype)


def mix_kernel(tokens_ref, own_ref, next_ref, prev_ref, next2_ref, prev2_ref, far_ref, above_ref, below_ref, out_ref):
    rows = tokens_ref.shape[0]
    total = own_ref[:rows]
    for ref in (next_ref, prev_ref, next2_ref, prev2_ref, far_ref, above_ref, below_ref):
        total = total + ref[:rows].astype(jnp.float32)
    out_ref[...] = (tokens_ref[...].astype(jnp.float32) + 0.5 * total).astype(out_ref.dtype)


def step(tokens, norm_gain, gate_master, up_master, down_master):
    copies = weight_copies(norm_gain, gate_master, up_master, down_master, lax.axis_size("fs"))
    packed = lax.all_to_all(copies, "fs", split_axis=0, concat_axis=0, tiled=True)
    spread = lax.all_gather(tokens, "zh", axis=0, tiled=True)
    rows, width = tokens.shape
    shapes = tuple(jax.ShapeDtypeStruct((k * rows, width), tokens.dtype) for k in (4, 2, 2))
    held, pair_above, pair_below = local(order_kernel, shapes, spread)
    from_next = move(held, -1)
    from_prev = move(held, 1)
    from_next2 = move(pair_above, -2)
    from_prev2 = move(pair_below, 2)

    partner = lax.ppermute(packed, "c", [(0, 1), (1, 0)])
    weights = (packed, partner)

    (ones_next,) = partial_sums((from_next,), weights, 1, jnp.bfloat16)
    to_next = move(ones_next, 1)
    (ones_prev,) = partial_sums((from_prev,), weights, 1, jnp.bfloat16)
    to_prev = move(ones_prev, -1)
    twos_next, twos_prev = partial_sums((from_next2, from_prev2), weights, 2, jnp.bfloat16)
    to_next2 = move(twos_next, 2)
    to_prev2 = move(twos_prev, -2)
    (own,) = partial_sums((held,), weights, 1, jnp.float32)

    block = jax.ShapeDtypeStruct(tokens.shape, jnp.bfloat16)
    (sum_far,) = local(lambda *refs: fold_kernel((((0, 1), (1, 1), (2, 1)),), *refs), (block,), own, to_next, to_prev)
    back_far = move(sum_far, 8)
    terms = (((0, 2), (1, 2), (2, 2), (3, 1)), ((0, 3), (1, 3), (2, 3), (4, 1)))
    sum_above, sum_below = local(lambda *refs: fold_kernel(terms, *refs), (block, block), own, to_next, to_prev, to_next2, to_prev2)
    back_above = move(sum_above, 4)
    back_below = move(sum_below, -4)
    (mixed,) = local(mix_kernel, (block,), tokens, own, to_next, to_prev, to_next2, to_prev2, back_far, back_above, back_below)
    return (mixed, *(packed[:, k].reshape(-1, packed.shape[-1]) for k in range(3)))


def solution(mesh):
    split = Mesh(mesh.devices.reshape(mesh.shape["fs"], 4, 4, 2), ROWS)
    placed = (P(ROWS, None), P("fs"), P("fs", TP), P("fs", TP), P("fs", TP))
    return jax.shard_map(
        step,
        mesh=split,
        in_specs=placed,
        out_specs=(P(ROWS, None), P(None, TP), P(None, TP), P(None, TP)),
        check_vma=False,
    )
```

```python
import jax
import jax.numpy as jnp
from jax import lax
from jax.experimental import pallas as pl
from jax.experimental.pallas import tpu as pltpu
from jax.sharding import Mesh
from jax.sharding import PartitionSpec as P


Z = ("zh", "zl")
TP = (*Z, "c")
ROWS = ("fs", *TP)
VMEM = pl.BlockSpec(memory_space=pltpu.VMEM)
PARAMS = pltpu.CompilerParams(vmem_limit_bytes=32 * 1024 * 1024)


def local(kernel, outs, *args, flops=0, transcendentals=0):
    moved = sum(a.size * a.dtype.itemsize for a in (*args, *outs))
    return pl.pallas_call(
        kernel,
        out_shape=outs,
        in_specs=[VMEM] * len(args),
        out_specs=tuple(VMEM for _ in outs),
        compiler_params=PARAMS,
        cost_estimate=pl.CostEstimate(flops=flops, bytes_accessed=moved, transcendentals=transcendentals),
    )(*args)


def move(array, by):
    planes = lax.axis_size(Z)
    return lax.ppermute(array, Z, [(i, (i + by) % planes) for i in range(planes)])


def copies_kernel(gain_hbm, gate_hbm, up_hbm, down_hbm, out_hbm, gain_ref, wide_ref, shard_ref, in_sems, out_sems):
    loads = [pltpu.make_async_copy(gain_hbm, gain_ref, in_sems.at[3])]
    for k, source in enumerate((gate_hbm, up_hbm, down_hbm)):
        loads.append(pltpu.make_async_copy(source, wide_ref.at[k], in_sems.at[k]))
    for load in loads:
        load.start()
    loads[0].wait()
    count = gate_hbm.shape[0]
    gain = jnp.transpose(jnp.broadcast_to(gain_ref[...], (count, count)))
    gain = jnp.concatenate([gain] * (gate_hbm.shape[1] // count), axis=1)
    stores = []
    for k in range(3):
        loads[1 + k].wait()
        value = wide_ref[k]
        shard_ref[k] = (value if k == 2 else gain * value).astype(jnp.bfloat16)
    for i in range(out_hbm.shape[0]):
        stores.append(pltpu.make_async_copy(shard_ref, out_hbm.at[i], out_sems.at[i]))
        stores[-1].start()
    for store in stores:
        store.wait()


def weight_copies(norm_gain, gate_master, up_master, down_master, count):
    shape = (3, *gate_master.shape)
    anywhere = pl.BlockSpec(memory_space=pltpu.HBM)
    return pl.pallas_call(
        copies_kernel,
        out_shape=jax.ShapeDtypeStruct((count, *shape), jnp.bfloat16),
        in_specs=[anywhere] * 4,
        out_specs=anywhere,
        scratch_shapes=[
            pltpu.VMEM((1, norm_gain.shape[0]), jnp.float32),
            pltpu.VMEM(shape, jnp.float32),
            pltpu.VMEM(shape, jnp.bfloat16),
            pltpu.SemaphoreType.DMA((4,)),
            pltpu.SemaphoreType.DMA((count,)),
        ],
        compiler_params=pltpu.CompilerParams(vmem_limit_bytes=66846720),
        cost_estimate=pl.CostEstimate(flops=1000000, bytes_accessed=4000000, transcendentals=0),
        name="prepare",
    )(norm_gain.reshape(1, -1), gate_master, up_master, down_master)


def order_kernel(from_ref, held_ref, above_ref, below_ref):
    rows = from_ref.shape[0] // 4
    here = lax.axis_index("zh")

    def block(by):
        return from_ref[pl.ds(pl.multiple_of((here + by) % 4 * rows, rows), rows)]

    own, above, below = block(0), block(1), block(3)
    for k, value in enumerate((own, block(2), above, below)):
        held_ref[k * rows : (k + 1) * rows] = value
    for ref, value in ((above_ref, above), (below_ref, below)):
        ref[:rows] = own
        ref[rows:] = value


def sums_kernel(count, *refs):
    rows_refs, (own_ref, partner_ref), out_refs = refs[:count], refs[count : count + 2], refs[count + 2 :]
    rows = jnp.concatenate([ref[...] for ref in rows_refs], axis=0)
    width = rows.shape[1]
    wide = rows.astype(jnp.float32)
    row_scale = lax.rsqrt(jnp.mean(wide * wide, axis=1, keepdims=True) + 1e-06)
    hidden = []
    for ref in (own_ref, partner_ref):
        gate = ref[:, 0].reshape(width, -1)
        up = ref[:, 1].reshape(width, -1)
        gate_proj = row_scale * jnp.dot(rows, gate, preferred_element_type=jnp.float32)
        up_proj = row_scale * jnp.dot(rows, up, preferred_element_type=jnp.float32)
        hidden.append((gate_proj / (1.0 + jnp.exp(-gate_proj)) * up_proj).astype(jnp.bfloat16))
    total = None
    for ref, part in zip((own_ref, partner_ref), hidden):
        down = ref[:, 2].reshape(width, -1)
        share = lax.dot_general(part, down, (((1,), (1,)), ((), ())), preferred_element_type=jnp.float32)
        total = share if total is None else total + share
    at = 0
    for ref in out_refs:
        ref[...] = total[at : at + ref.shape[0]].astype(ref.dtype)
        at += ref.shape[0]


def partial_sums(parts, weights, outs, dtype):
    units = 2 * weights[0].shape[-1]
    count, width = sum(p.shape[0] for p in parts), parts[0].shape[1]
    return local(
        lambda *refs: sums_kernel(len(parts), *refs),
        tuple(jax.ShapeDtypeStruct((count // outs, width), dtype) for _ in range(outs)),
        *parts,
        *weights,
        flops=6 * count * width * units,
        transcendentals=count * units,
    )


def fold_far_kernel(own_ref, next_ref, prev_ref, up_ref, down_ref):
    half = up_ref.shape[0]
    rows = 2 * half
    for ref, at in ((up_ref, rows), (down_ref, rows + half)):
        total = own_ref[at : at + half]
        for other in (next_ref, prev_ref):
            total = total + other[at : at + half].astype(jnp.float32)
        ref[...] = total.astype(ref.dtype)


def fold_near_kernel(own_ref, next_ref, prev_ref, next2_ref, prev2_ref, up_ref, down_ref, above_ref, below_ref):
    rows = above_ref.shape[0]
    half = rows // 2
    for out_ref, block, second_ref, half_ref, at in ((above_ref, 2, next2_ref, up_ref, 0), (below_ref, 3, prev2_ref, down_ref, half)):
        for part in (0, half):
            lower = block * rows + part
            total = own_ref[lower : lower + half] + second_ref[rows + part : rows + part + half].astype(jnp.float32)
            for other in (next_ref, prev_ref):
                total = total + other[lower : lower + half].astype(jnp.float32)
            if part == at:
                total = total + half_ref[...].astype(jnp.float32)
            out_ref[part : part + half] = total.astype(out_ref.dtype)


def mix_kernel(tokens_ref, own_ref, next_ref, prev_ref, next2_ref, prev2_ref, above_ref, below_ref, out_ref):
    rows = tokens_ref.shape[0]
    total = own_ref[:rows]
    for ref in (next_ref, prev_ref, next2_ref, prev2_ref, above_ref, below_ref):
        total = total + ref[:rows].astype(jnp.float32)
    out_ref[...] = (tokens_ref[...].astype(jnp.float32) + 0.5 * total).astype(out_ref.dtype)


def step(tokens, norm_gain, gate_master, up_master, down_master):
    copies = weight_copies(norm_gain, gate_master, up_master, down_master, lax.axis_size("fs"))
    packed = lax.all_to_all(copies, "fs", split_axis=0, concat_axis=0, tiled=True)
    spread = lax.all_gather(tokens, "zh", axis=0, tiled=True)
    rows, width = tokens.shape
    shapes = tuple(jax.ShapeDtypeStruct((k * rows, width), tokens.dtype) for k in (4, 2, 2))
    held, pair_above, pair_below = local(order_kernel, shapes, spread)
    from_next = move(held, -1)
    from_prev = move(held, 1)
    from_next2 = move(pair_above, -2)
    from_prev2 = move(pair_below, 2)

    partner = lax.ppermute(packed, "c", [(0, 1), (1, 0)])
    weights = (packed, partner)

    (ones_next,) = partial_sums((from_next,), weights, 1, jnp.bfloat16)
    to_next = move(ones_next, 1)
    (ones_prev,) = partial_sums((from_prev,), weights, 1, jnp.bfloat16)
    to_prev = move(ones_prev, -1)
    twos_next, twos_prev = partial_sums((from_next2, from_prev2), weights, 2, jnp.bfloat16)
    to_next2 = move(twos_next, 2)
    to_prev2 = move(twos_prev, -2)
    (own,) = partial_sums((held,), weights, 1, jnp.float32)

    block = jax.ShapeDtypeStruct((rows, width), jnp.bfloat16)
    part = jax.ShapeDtypeStruct((rows // 2, width), jnp.bfloat16)
    far_up, far_down = local(fold_far_kernel, (part, part), own, to_next, to_prev)
    back_up = move(far_up, 4)
    back_down = move(far_down, -4)
    received = (own, to_next, to_prev, to_next2, to_prev2)
    sum_above, sum_below = local(fold_near_kernel, (block, block), *received, back_up, back_down)
    back_above = move(sum_above, 4)
    back_below = move(sum_below, -4)
    (mixed,) = local(mix_kernel, (block,), tokens, *received, back_above, back_below)
    return (mixed, *(packed[:, k].reshape(-1, packed.shape[-1]) for k in range(3)))


def solution(mesh):
    split = Mesh(mesh.devices.reshape(mesh.shape["fs"], 4, 4, 2), ROWS)
    placed = (P(ROWS, None), P("fs"), P("fs", TP), P("fs", TP), P("fs", TP))
    return jax.shard_map(
        step,
        mesh=split,
        in_specs=placed,
        out_specs=(P(ROWS, None), P(None, TP), P(None, TP), P(None, TP)),
        check_vma=False,
    )
```

```python
import jax
import jax.numpy as jnp
from jax import lax
from jax.experimental import pallas as pl
from jax.experimental.pallas import tpu as pltpu
from jax.sharding import Mesh
from jax.sharding import PartitionSpec as P


Z = ("zh", "zl")
TP = (*Z, "c")
ROWS = ("fs", *TP)
VMEM = pl.BlockSpec(memory_space=pltpu.VMEM)
PARAMS = pltpu.CompilerParams(vmem_limit_bytes=32 * 1024 * 1024)


def local(kernel, outs, *args, flops=0, transcendentals=0):
    moved = sum(a.size * a.dtype.itemsize for a in (*args, *outs))
    return pl.pallas_call(
        kernel,
        out_shape=outs,
        in_specs=[VMEM] * len(args),
        out_specs=tuple(VMEM for _ in outs),
        compiler_params=PARAMS,
        cost_estimate=pl.CostEstimate(flops=flops, bytes_accessed=moved, transcendentals=transcendentals),
    )(*args)


def move(array, by):
    planes = lax.axis_size(Z)
    return lax.ppermute(array, Z, [(i, (i + by) % planes) for i in range(planes)])


def move_by_core(array, by):
    planes = lax.axis_size(Z)
    pairs = [(2 * i + c, 2 * ((i + way * by) % planes) + c) for c, way in ((0, 1), (1, -1)) for i in range(planes)]
    return lax.ppermute(array, TP, pairs)


def copies_kernel(gain_hbm, gate_hbm, up_hbm, down_hbm, out_hbm, gain_ref, wide_ref, shard_ref, in_sems, out_sems):
    loads = [pltpu.make_async_copy(gain_hbm, gain_ref, in_sems.at[3])]
    for k, source in enumerate((gate_hbm, up_hbm, down_hbm)):
        loads.append(pltpu.make_async_copy(source, wide_ref.at[k], in_sems.at[k]))
    for load in loads:
        load.start()
    loads[0].wait()
    count = gate_hbm.shape[0]
    gain = jnp.transpose(jnp.broadcast_to(gain_ref[...], (count, count)))
    gain = jnp.concatenate([gain] * (gate_hbm.shape[1] // count), axis=1)
    stores = []
    for k in range(3):
        loads[1 + k].wait()
        value = wide_ref[k]
        shard_ref[k] = (value if k == 2 else gain * value).astype(jnp.bfloat16)
    for i in range(out_hbm.shape[0]):
        stores.append(pltpu.make_async_copy(shard_ref, out_hbm.at[i], out_sems.at[i]))
        stores[-1].start()
    for store in stores:
        store.wait()


def weight_copies(norm_gain, gate_master, up_master, down_master, count):
    shape = (3, *gate_master.shape)
    anywhere = pl.BlockSpec(memory_space=pltpu.HBM)
    return pl.pallas_call(
        copies_kernel,
        out_shape=jax.ShapeDtypeStruct((count, *shape), jnp.bfloat16),
        in_specs=[anywhere] * 4,
        out_specs=anywhere,
        scratch_shapes=[
            pltpu.VMEM((1, norm_gain.shape[0]), jnp.float32),
            pltpu.VMEM(shape, jnp.float32),
            pltpu.VMEM(shape, jnp.bfloat16),
            pltpu.SemaphoreType.DMA((4,)),
            pltpu.SemaphoreType.DMA((count,)),
        ],
        compiler_params=pltpu.CompilerParams(vmem_limit_bytes=66846720),
        cost_estimate=pl.CostEstimate(flops=1000000, bytes_accessed=4000000, transcendentals=0),
        name="prepare",
    )(norm_gain.reshape(1, -1), gate_master, up_master, down_master)


def order_kernel(from_ref, held_ref):
    rows = from_ref.shape[0] // 4
    here = lax.axis_index("zh")
    for k, by in enumerate((0, 2, 1, 3)):
        held_ref[k * rows : (k + 1) * rows] = from_ref[pl.ds(pl.multiple_of((here + by) % 4 * rows, rows), rows)]


def plane_twos(ref):
    rows = ref.shape[0] // 4
    core = lax.axis_index("c")
    return [ref[pl.ds(pl.multiple_of(jnp.where(core == 0, up, down) * rows, rows), rows)] for up, down in ((0, 2), (2, 1), (3, 0), (1, 3))]


def sums_kernel(count, twos, *refs):
    rows_refs, (own_ref, partner_ref), out_refs = refs[:count], refs[count : count + 2], refs[count + 2 :]
    blocks = [ref[...] for ref in rows_refs[: count - twos]]
    for ref in rows_refs[count - twos :]:
        blocks += plane_twos(ref)
    rows = jnp.concatenate(blocks, axis=0)
    width = rows.shape[1]
    wide = rows.astype(jnp.float32)
    row_scale = lax.rsqrt(jnp.mean(wide * wide, axis=1, keepdims=True) + 1e-06)
    hidden = []
    for ref in (own_ref, partner_ref):
        gate = ref[:, 0].reshape(width, -1)
        up = ref[:, 1].reshape(width, -1)
        gate_proj = row_scale * jnp.dot(rows, gate, preferred_element_type=jnp.float32)
        up_proj = row_scale * jnp.dot(rows, up, preferred_element_type=jnp.float32)
        hidden.append((gate_proj / (1.0 + jnp.exp(-gate_proj)) * up_proj).astype(jnp.bfloat16))
    total = None
    for ref, part in zip((own_ref, partner_ref), hidden):
        down = ref[:, 2].reshape(width, -1)
        share = lax.dot_general(part, down, (((1,), (1,)), ((), ())), preferred_element_type=jnp.float32)
        total = share if total is None else total + share
    at = 0
    for ref in out_refs:
        ref[...] = total[at : at + ref.shape[0]].astype(ref.dtype)
        at += ref.shape[0]


def partial_sums(parts, twos, weights, counts, dtype):
    units = 2 * weights[0].shape[-1]
    count, width = sum(counts), parts[0].shape[1]
    return local(
        lambda *refs: sums_kernel(len(parts), twos, *refs),
        tuple(jax.ShapeDtypeStruct((k, width), dtype) for k in counts),
        *parts,
        *weights,
        flops=6 * count * width * units,
        transcendentals=count * units,
    )


def fold_far_kernel(own_ref, next_ref, prev_ref, far_ref):
    rows = far_ref.shape[0]
    total = own_ref[rows : 2 * rows]
    for other in (next_ref, prev_ref):
        total = total + other[rows : 2 * rows].astype(jnp.float32)
    far_ref[...] = total.astype(far_ref.dtype)


def fold_near_kernel(own_ref, next_ref, prev_ref, next2_ref, prev2_ref, far_ref, above_ref, below_ref):
    rows = above_ref.shape[0]
    core = lax.axis_index("c")
    far = far_ref[...].astype(jnp.float32)
    for out_ref, block, second_ref, way in ((above_ref, 2, next2_ref, 0), (below_ref, 3, prev2_ref, 1)):
        total = own_ref[block * rows : (block + 1) * rows] + second_ref[rows:].astype(jnp.float32)
        for other in (next_ref, prev_ref):
            total = total + other[block * rows : (block + 1) * rows].astype(jnp.float32)
        out_ref[...] = (total + jnp.where(core == way, far, 0.0)).astype(out_ref.dtype)


def mix_kernel(tokens_ref, own_ref, next_ref, prev_ref, next2_ref, prev2_ref, above_ref, below_ref, out_ref):
    rows = tokens_ref.shape[0]
    total = own_ref[:rows]
    for ref in (next_ref, prev_ref, next2_ref, prev2_ref, above_ref, below_ref):
        total = total + ref[:rows].astype(jnp.float32)
    out_ref[...] = (tokens_ref[...].astype(jnp.float32) + 0.5 * total).astype(out_ref.dtype)


def step(tokens, norm_gain, gate_master, up_master, down_master):
    copies = weight_copies(norm_gain, gate_master, up_master, down_master, lax.axis_size("fs"))
    packed = lax.all_to_all(copies, "fs", split_axis=0, concat_axis=0, tiled=True)
    spread = lax.all_gather(tokens, "zh", axis=0, tiled=True)
    rows, width = tokens.shape
    (held,) = local(order_kernel, (jax.ShapeDtypeStruct((4 * rows, width), tokens.dtype),), spread)
    from_next = move(held, -1)
    from_prev = move(held, 1)
    from_twos = move_by_core(held, -2)

    partner = lax.ppermute(packed, "c", [(0, 1), (1, 0)])
    weights = (packed, partner)

    counts = (4 * rows, 4 * rows, 2 * rows, 2 * rows)
    for_next, for_prev, for_next2, for_prev2 = partial_sums((from_next, from_prev, from_twos), 1, weights, counts, jnp.bfloat16)
    to_next = move(for_next, 1)
    to_prev = move(for_prev, -1)
    to_next2 = move(for_next2, 2)
    to_prev2 = move(for_prev2, -2)
    (own,) = partial_sums((held,), 0, weights, (4 * rows,), jnp.float32)

    block = jax.ShapeDtypeStruct((rows, width), jnp.bfloat16)
    (sum_far,) = local(fold_far_kernel, (block,), own, to_next, to_prev)
    back_far = move_by_core(sum_far, 4)
    received = (own, to_next, to_prev, to_next2, to_prev2)
    sum_above, sum_below = local(fold_near_kernel, (block, block), *received, back_far)
    back_above = move(sum_above, 4)
    back_below = move(sum_below, -4)
    (mixed,) = local(mix_kernel, (block,), tokens, *received, back_above, back_below)
    return (mixed, *(packed[:, k].reshape(-1, packed.shape[-1]) for k in range(3)))


def solution(mesh):
    split = Mesh(mesh.devices.reshape(mesh.shape["fs"], 4, 4, 2), ROWS)
    placed = (P(ROWS, None), P("fs"), P("fs", TP), P("fs", TP), P("fs", TP))
    return jax.shard_map(
        step,
        mesh=split,
        in_specs=placed,
        out_specs=(P(ROWS, None), P(None, TP), P(None, TP), P(None, TP)),
        check_vma=False,
    )
```

```python
import jax
import jax.numpy as jnp
from jax import lax
from jax.experimental import pallas as pl
from jax.experimental.pallas import tpu as pltpu
from jax.sharding import Mesh
from jax.sharding import PartitionSpec as P


Z = ("zh", "zl")
TP = (*Z, "c")
ROWS = ("fs", *TP)
VMEM = pl.BlockSpec(memory_space=pltpu.VMEM)
PARAMS = pltpu.CompilerParams(vmem_limit_bytes=32 * 1024 * 1024)


def local(kernel, outs, *args, flops=0, transcendentals=0):
    moved = sum(a.size * a.dtype.itemsize for a in (*args, *outs))
    return pl.pallas_call(
        kernel,
        out_shape=outs,
        in_specs=[VMEM] * len(args),
        out_specs=tuple(VMEM for _ in outs),
        compiler_params=PARAMS,
        cost_estimate=pl.CostEstimate(flops=flops, bytes_accessed=moved, transcendentals=transcendentals),
    )(*args)


def move(array, by):
    planes = lax.axis_size(Z)
    return lax.ppermute(array, Z, [(i, (i + by) % planes) for i in range(planes)])


def move_by_core(array, by):
    planes = lax.axis_size(Z)
    pairs = [(2 * i + c, 2 * ((i + way * by) % planes) + c) for c, way in ((0, 1), (1, -1)) for i in range(planes)]
    return lax.ppermute(array, TP, pairs)


def copies_kernel(gain_hbm, gate_hbm, up_hbm, down_hbm, out_hbm, gain_ref, wide_ref, shard_ref, in_sems, out_sems):
    loads = [pltpu.make_async_copy(gain_hbm, gain_ref, in_sems.at[3])]
    for k, source in enumerate((gate_hbm, up_hbm, down_hbm)):
        loads.append(pltpu.make_async_copy(source, wide_ref.at[k], in_sems.at[k]))
    for load in loads:
        load.start()
    loads[0].wait()
    count = gate_hbm.shape[0]
    gain = jnp.transpose(jnp.broadcast_to(gain_ref[...], (count, count)))
    gain = jnp.concatenate([gain] * (gate_hbm.shape[1] // count), axis=1)
    stores = []
    for k in range(3):
        loads[1 + k].wait()
        value = wide_ref[k]
        shard_ref[k] = (value if k == 2 else gain * value).astype(jnp.bfloat16)
    for i in range(out_hbm.shape[0]):
        stores.append(pltpu.make_async_copy(shard_ref, out_hbm.at[i], out_sems.at[i]))
        stores[-1].start()
    for store in stores:
        store.wait()


def weight_copies(norm_gain, gate_master, up_master, down_master, count):
    shape = (3, *gate_master.shape)
    anywhere = pl.BlockSpec(memory_space=pltpu.HBM)
    return pl.pallas_call(
        copies_kernel,
        out_shape=jax.ShapeDtypeStruct((count, *shape), jnp.bfloat16),
        in_specs=[anywhere] * 4,
        out_specs=anywhere,
        scratch_shapes=[
            pltpu.VMEM((1, norm_gain.shape[0]), jnp.float32),
            pltpu.VMEM(shape, jnp.float32),
            pltpu.VMEM(shape, jnp.bfloat16),
            pltpu.SemaphoreType.DMA((4,)),
            pltpu.SemaphoreType.DMA((count,)),
        ],
        compiler_params=pltpu.CompilerParams(vmem_limit_bytes=66846720),
        cost_estimate=pl.CostEstimate(flops=1000000, bytes_accessed=4000000, transcendentals=0),
        name="prepare",
    )(norm_gain.reshape(1, -1), gate_master, up_master, down_master)


def order_kernel(from_ref, held_ref):
    rows = from_ref.shape[0] // 4
    here = lax.axis_index("zh")
    for k, by in enumerate((0, 2, 1, 3)):
        held_ref[k * rows : (k + 1) * rows] = from_ref[pl.ds(pl.multiple_of((here + by) % 4 * rows, rows), rows)]


def plane_twos(ref):
    rows = ref.shape[0] // 4
    core = lax.axis_index("c")
    return [ref[pl.ds(pl.multiple_of(jnp.where(core == 0, up, down) * rows, rows), rows)] for up, down in ((0, 2), (2, 1), (3, 0), (1, 3))]


def sums_kernel(count, twos, *refs):
    rows_refs, (own_ref, partner_ref), out_refs = refs[:count], refs[count : count + 2], refs[count + 2 :]
    blocks = [ref[...] for ref in rows_refs[: count - twos]]
    for ref in rows_refs[count - twos :]:
        blocks += plane_twos(ref)
    rows = jnp.concatenate(blocks, axis=0)
    width = rows.shape[1]
    wide = rows.astype(jnp.float32)
    row_scale = lax.rsqrt(jnp.mean(wide * wide, axis=1, keepdims=True) + 1e-06)
    hidden = []
    for ref in (own_ref, partner_ref):
        gate = ref[:, 0].reshape(width, -1)
        up = ref[:, 1].reshape(width, -1)
        gate_proj = row_scale * jnp.dot(rows, gate, preferred_element_type=jnp.float32)
        up_proj = row_scale * jnp.dot(rows, up, preferred_element_type=jnp.float32)
        hidden.append((gate_proj / (1.0 + jnp.exp(-gate_proj)) * up_proj).astype(jnp.bfloat16))
    total = None
    for ref, part in zip((own_ref, partner_ref), hidden):
        down = ref[:, 2].reshape(width, -1)
        share = lax.dot_general(part, down, (((1,), (1,)), ((), ())), preferred_element_type=jnp.float32)
        total = share if total is None else total + share
    at = 0
    for ref in out_refs:
        ref[...] = total[at : at + ref.shape[0]].astype(ref.dtype)
        at += ref.shape[0]


def partial_sums(parts, twos, weights, counts, dtype):
    units = 2 * weights[0].shape[-1]
    count, width = sum(counts), parts[0].shape[1]
    return local(
        lambda *refs: sums_kernel(len(parts), twos, *refs),
        tuple(jax.ShapeDtypeStruct((k, width), dtype) for k in counts),
        *parts,
        *weights,
        flops=6 * count * width * units,
        transcendentals=count * units,
    )


def fold_far_kernel(own_ref, next_ref, prev_ref, far_ref):
    rows = far_ref.shape[0]
    total = own_ref[rows : 2 * rows]
    for other in (next_ref, prev_ref):
        total = total + other[rows : 2 * rows].astype(jnp.float32)
    far_ref[...] = total.astype(far_ref.dtype)


def fold_near_kernel(way, own_ref, next_ref, prev_ref, next2_ref, prev2_ref, *refs):
    *far_refs, out_ref = refs
    rows = out_ref.shape[0]
    up = lax.axis_index("c") == way
    lower = pl.multiple_of(jnp.where(up, 2, 3) * rows, rows)
    total = own_ref[pl.ds(lower, rows)] + jnp.where(up, next2_ref[rows:].astype(jnp.float32), prev2_ref[rows:].astype(jnp.float32))
    for other in (next_ref, prev_ref):
        total = total + other[pl.ds(lower, rows)].astype(jnp.float32)
    for ref in far_refs:
        total = total + ref[...].astype(jnp.float32)
    out_ref[...] = total.astype(out_ref.dtype)


def mix_kernel(tokens_ref, own_ref, next_ref, prev_ref, next2_ref, prev2_ref, above_ref, below_ref, out_ref):
    rows = tokens_ref.shape[0]
    total = own_ref[:rows]
    for ref in (next_ref, prev_ref, next2_ref, prev2_ref, above_ref, below_ref):
        total = total + ref[:rows].astype(jnp.float32)
    out_ref[...] = (tokens_ref[...].astype(jnp.float32) + 0.5 * total).astype(out_ref.dtype)


def step(tokens, norm_gain, gate_master, up_master, down_master):
    copies = weight_copies(norm_gain, gate_master, up_master, down_master, lax.axis_size("fs"))
    packed = lax.all_to_all(copies, "fs", split_axis=0, concat_axis=0, tiled=True)
    spread = lax.all_gather(tokens, "zh", axis=0, tiled=True)
    rows, width = tokens.shape
    (held,) = local(order_kernel, (jax.ShapeDtypeStruct((4 * rows, width), tokens.dtype),), spread)
    from_next = move(held, -1)
    from_prev = move(held, 1)
    from_twos = move_by_core(held, -2)

    partner = lax.ppermute(packed, "c", [(0, 1), (1, 0)])
    weights = (packed, partner)

    for_next, for_prev = partial_sums((from_next, from_prev), 0, weights, (4 * rows, 4 * rows), jnp.bfloat16)
    to_next = move(for_next, 1)
    to_prev = move(for_prev, -1)
    for_next2, for_prev2 = partial_sums((from_twos,), 1, weights, (2 * rows, 2 * rows), jnp.bfloat16)
    to_next2 = move(for_next2, 2)
    to_prev2 = move(for_prev2, -2)
    (own,) = partial_sums((held,), 0, weights, (4 * rows,), jnp.float32)

    block = jax.ShapeDtypeStruct((rows, width), jnp.bfloat16)
    (sum_far,) = local(fold_far_kernel, (block,), own, to_next, to_prev)
    back_far = move_by_core(sum_far, 4)
    received = (own, to_next, to_prev, to_next2, to_prev2)
    (sum_plain,) = local(lambda *refs: fold_near_kernel(1, *refs), (block,), *received)
    back_plain = move_by_core(sum_plain, -4)
    (sum_joint,) = local(lambda *refs: fold_near_kernel(0, *refs), (block,), *received, back_far)
    back_joint = move_by_core(sum_joint, 4)
    (mixed,) = local(mix_kernel, (block,), tokens, *received, back_plain, back_joint)
    return (mixed, *(packed[:, k].reshape(-1, packed.shape[-1]) for k in range(3)))


def solution(mesh):
    split = Mesh(mesh.devices.reshape(mesh.shape["fs"], 4, 4, 2), ROWS)
    placed = (P(ROWS, None), P("fs"), P("fs", TP), P("fs", TP), P("fs", TP))
    return jax.shard_map(
        step,
        mesh=split,
        in_specs=placed,
        out_specs=(P(ROWS, None), P(None, TP), P(None, TP), P(None, TP)),
        check_vma=False,
    )
```

```python
import jax
import jax.numpy as jnp
from jax import lax
from jax.experimental import pallas as pl
from jax.experimental.pallas import tpu as pltpu
from jax.sharding import Mesh
from jax.sharding import PartitionSpec as P


Z = ("zh", "zl")
TP = (*Z, "c")
ROWS = ("fs", *TP)
VMEM = pl.BlockSpec(memory_space=pltpu.VMEM)
PARAMS = pltpu.CompilerParams(vmem_limit_bytes=32 * 1024 * 1024)


def local(kernel, outs, *args, flops=0, transcendentals=0):
    moved = sum(a.size * a.dtype.itemsize for a in (*args, *outs))
    return pl.pallas_call(
        kernel,
        out_shape=outs,
        in_specs=[VMEM] * len(args),
        out_specs=tuple(VMEM for _ in outs),
        compiler_params=PARAMS,
        cost_estimate=pl.CostEstimate(flops=flops, bytes_accessed=moved, transcendentals=transcendentals),
    )(*args)


def move(array, by):
    planes = lax.axis_size(Z)
    return lax.ppermute(array, Z, [(i, (i + by) % planes) for i in range(planes)])


def move_by_core(array, by):
    planes = lax.axis_size(Z)
    pairs = [(2 * i + c, 2 * ((i + way * by) % planes) + c) for c, way in ((0, 1), (1, -1)) for i in range(planes)]
    return lax.ppermute(array, TP, pairs)


def copies_kernel(gain_hbm, gate_hbm, up_hbm, down_hbm, out_hbm, gain_ref, wide_ref, shard_ref, in_sems, out_sems):
    loads = [pltpu.make_async_copy(gain_hbm, gain_ref, in_sems.at[3])]
    for k, source in enumerate((gate_hbm, up_hbm, down_hbm)):
        loads.append(pltpu.make_async_copy(source, wide_ref.at[k], in_sems.at[k]))
    for load in loads:
        load.start()
    loads[0].wait()
    count = gate_hbm.shape[0]
    gain = jnp.transpose(jnp.broadcast_to(gain_ref[...], (count, count)))
    gain = jnp.concatenate([gain] * (gate_hbm.shape[1] // count), axis=1)
    stores = []
    for k in range(3):
        loads[1 + k].wait()
        value = wide_ref[k]
        shard_ref[k] = (value if k == 2 else gain * value).astype(jnp.bfloat16)
    for i in range(out_hbm.shape[0]):
        stores.append(pltpu.make_async_copy(shard_ref, out_hbm.at[i], out_sems.at[i]))
        stores[-1].start()
    for store in stores:
        store.wait()


def weight_copies(norm_gain, gate_master, up_master, down_master, count):
    shape = (3, *gate_master.shape)
    anywhere = pl.BlockSpec(memory_space=pltpu.HBM)
    return pl.pallas_call(
        copies_kernel,
        out_shape=jax.ShapeDtypeStruct((count, *shape), jnp.bfloat16),
        in_specs=[anywhere] * 4,
        out_specs=anywhere,
        scratch_shapes=[
            pltpu.VMEM((1, norm_gain.shape[0]), jnp.float32),
            pltpu.VMEM(shape, jnp.float32),
            pltpu.VMEM(shape, jnp.bfloat16),
            pltpu.SemaphoreType.DMA((4,)),
            pltpu.SemaphoreType.DMA((count,)),
        ],
        compiler_params=pltpu.CompilerParams(vmem_limit_bytes=66846720),
        cost_estimate=pl.CostEstimate(flops=1000000, bytes_accessed=4000000, transcendentals=0),
        name="prepare",
    )(norm_gain.reshape(1, -1), gate_master, up_master, down_master)


def blocks_of(ref, by, order):
    rows = ref.shape[0] // 4
    plane = lax.rem(lax.axis_index("zh") * 4 + lax.axis_index("zl") + by + 16, 16)
    first = lax.div(plane, 4)
    return [ref[pl.ds(pl.multiple_of(lax.rem(first + j, 4) * rows, rows), rows)] for j in order]


def blocks_of_twos(ref):
    up = lax.axis_index("c") == 0
    return blocks_of(ref, jnp.where(up, 2, -2), [jnp.where(up, a, b) for a, b in ((0, 1), (1, 2), (3, 0), (2, 3))])


def share(rows, weights_ref):
    width = rows.shape[1]
    gate, up, down = (weights_ref[:, k].reshape(width, -1) for k in range(3))
    wide = rows.astype(jnp.float32)
    row_scale = lax.rsqrt(jnp.mean(wide * wide, axis=1, keepdims=True) + 1e-06)
    gate_proj = row_scale * jnp.dot(rows, gate, preferred_element_type=jnp.float32)
    up_proj = row_scale * jnp.dot(rows, up, preferred_element_type=jnp.float32)
    hidden = (gate_proj / (1.0 + jnp.exp(-gate_proj)) * up_proj).astype(jnp.bfloat16)
    return lax.dot_general(hidden, down, (((1,), (1,)), ((), ())), preferred_element_type=jnp.float32)


def sums_kernel(orders, weights, begun, *refs):
    count = len(orders)
    rows_refs, weights_refs, refs = refs[:count], refs[count : count + weights], refs[count + weights :]
    begun_refs, out_refs = refs[:begun], refs[begun:]
    rows = jnp.concatenate([block for order, ref in zip(orders, rows_refs) for block in order(ref)], axis=0)
    total = begun_refs[0][...] if begun else None
    for ref in weights_refs:
        added = share(rows, ref)
        total = added if total is None else total + added
    at = 0
    for ref in out_refs:
        ref[...] = total[at : at + ref.shape[0]].astype(ref.dtype)
        at += ref.shape[0]


def partial_sums(parts, orders, weights, counts, dtype, begun=()):
    units = len(weights) * weights[0].shape[-1]
    count, width = sum(counts), parts[0].shape[1]
    return local(
        lambda *refs: sums_kernel(orders, len(weights), len(begun), *refs),
        tuple(jax.ShapeDtypeStruct((k, width), dtype) for k in counts),
        *parts,
        *weights,
        *begun,
        flops=6 * count * width * units,
        transcendentals=count * units,
    )


def fold_far_kernel(own_ref, next_ref, prev_ref, far_ref):
    rows = far_ref.shape[0]
    total = own_ref[rows : 2 * rows]
    for other in (next_ref, prev_ref):
        total = total + other[rows : 2 * rows].astype(jnp.float32)
    far_ref[...] = total.astype(far_ref.dtype)


def fold_near_kernel(way, own_ref, next_ref, prev_ref, next2_ref, prev2_ref, *refs):
    *far_refs, out_ref = refs
    rows = out_ref.shape[0]
    up = lax.axis_index("c") == way
    lower = pl.multiple_of(jnp.where(up, 2, 3) * rows, rows)
    total = own_ref[pl.ds(lower, rows)] + jnp.where(up, next2_ref[rows:].astype(jnp.float32), prev2_ref[rows:].astype(jnp.float32))
    for other in (next_ref, prev_ref):
        total = total + other[pl.ds(lower, rows)].astype(jnp.float32)
    for ref in far_refs:
        total = total + ref[...].astype(jnp.float32)
    out_ref[...] = total.astype(out_ref.dtype)


def mix_kernel(tokens_ref, own_ref, next_ref, prev_ref, next2_ref, prev2_ref, above_ref, below_ref, out_ref):
    rows = tokens_ref.shape[0]
    total = own_ref[:rows]
    for ref in (next_ref, prev_ref, next2_ref, prev2_ref, above_ref, below_ref):
        total = total + ref[:rows].astype(jnp.float32)
    out_ref[...] = (tokens_ref[...].astype(jnp.float32) + 0.5 * total).astype(out_ref.dtype)


def step(tokens, norm_gain, gate_master, up_master, down_master):
    copies = weight_copies(norm_gain, gate_master, up_master, down_master, lax.axis_size("fs"))
    packed = lax.all_to_all(copies, "fs", split_axis=0, concat_axis=0, tiled=True)
    held = lax.all_gather(tokens, "zh", axis=0, tiled=True)
    rows, width = tokens.shape
    from_next = move(held, -1)
    from_prev = move(held, 1)
    from_twos = move_by_core(held, -2)

    partner = lax.ppermute(packed, "c", [(0, 1), (1, 0)])
    weights = (packed, partner)

    def around(by):
        return lambda ref: blocks_of(ref, by, (0, 2, 1, 3))

    sides, orders = (from_next, from_prev), (around(1), around(-1))
    half = partial_sums(sides, orders, weights[:1], (8 * rows,), jnp.float32)
    for_next, for_prev = partial_sums(sides, orders, weights[1:], (4 * rows, 4 * rows), jnp.bfloat16, half)
    to_next = move(for_next, 1)
    to_prev = move(for_prev, -1)
    for_next2, for_prev2 = partial_sums((from_twos,), (blocks_of_twos,), weights, (2 * rows, 2 * rows), jnp.bfloat16)
    to_next2 = move(for_next2, 2)
    to_prev2 = move(for_prev2, -2)
    (own,) = partial_sums((held,), (around(0),), weights, (4 * rows,), jnp.float32)

    block = jax.ShapeDtypeStruct((rows, width), jnp.bfloat16)
    (sum_far,) = local(fold_far_kernel, (block,), own, to_next, to_prev)
    back_far = move_by_core(sum_far, 4)
    received = (own, to_next, to_prev, to_next2, to_prev2)
    (sum_plain,) = local(lambda *refs: fold_near_kernel(1, *refs), (block,), *received)
    back_plain = move_by_core(sum_plain, -4)
    (sum_joint,) = local(lambda *refs: fold_near_kernel(0, *refs), (block,), *received, back_far)
    back_joint = move_by_core(sum_joint, 4)
    (mixed,) = local(mix_kernel, (block,), tokens, *received, back_plain, back_joint)
    return (mixed, *(packed[:, k].reshape(-1, packed.shape[-1]) for k in range(3)))


def solution(mesh):
    split = Mesh(mesh.devices.reshape(mesh.shape["fs"], 4, 4, 2), ROWS)
    placed = (P(ROWS, None), P("fs"), P("fs", TP), P("fs", TP), P("fs", TP))
    return jax.shard_map(
        step,
        mesh=split,
        in_specs=placed,
        out_specs=(P(ROWS, None), P(None, TP), P(None, TP), P(None, TP)),
        check_vma=False,
    )
```

```python
import jax
import jax.numpy as jnp
from jax import lax
from jax.experimental import pallas as pl
from jax.experimental.pallas import tpu as pltpu
from jax.sharding import Mesh
from jax.sharding import PartitionSpec as P


Z = ("zh", "zl")
TP = (*Z, "c")
ROWS = ("fs", *TP)
VMEM = pl.BlockSpec(memory_space=pltpu.VMEM)
PARAMS = pltpu.CompilerParams(vmem_limit_bytes=32 * 1024 * 1024)


def local(kernel, outs, *args, flops=0, transcendentals=0):
    moved = sum(a.size * a.dtype.itemsize for a in (*args, *outs))
    return pl.pallas_call(
        kernel,
        out_shape=outs,
        in_specs=[VMEM] * len(args),
        out_specs=tuple(VMEM for _ in outs),
        compiler_params=PARAMS,
        cost_estimate=pl.CostEstimate(flops=flops, bytes_accessed=moved, transcendentals=transcendentals),
    )(*args)


def move(array, by):
    planes = lax.axis_size(Z)
    return lax.ppermute(array, Z, [(i, (i + by) % planes) for i in range(planes)])


def move_by_core(array, by):
    planes = lax.axis_size(Z)
    pairs = [(2 * i + c, 2 * ((i + way * by) % planes) + c) for c, way in ((0, 1), (1, -1)) for i in range(planes)]
    return lax.ppermute(array, TP, pairs)


def copies_kernel(gain_hbm, gate_hbm, up_hbm, down_hbm, out_hbm, gain_ref, wide_ref, shard_ref, in_sems, out_sems):
    loads = [pltpu.make_async_copy(gain_hbm, gain_ref, in_sems.at[3])]
    for k, source in enumerate((gate_hbm, up_hbm, down_hbm)):
        loads.append(pltpu.make_async_copy(source, wide_ref.at[k], in_sems.at[k]))
    for load in loads:
        load.start()
    loads[0].wait()
    count = gate_hbm.shape[0]
    gain = jnp.transpose(jnp.broadcast_to(gain_ref[...], (count, count)))
    gain = jnp.concatenate([gain] * (gate_hbm.shape[1] // count), axis=1)
    stores = []
    for k in range(3):
        loads[1 + k].wait()
        value = wide_ref[k]
        shard_ref[k] = (value if k == 2 else gain * value).astype(jnp.bfloat16)
    for i in range(out_hbm.shape[0]):
        stores.append(pltpu.make_async_copy(shard_ref, out_hbm.at[i], out_sems.at[i]))
        stores[-1].start()
    for store in stores:
        store.wait()


def weight_copies(norm_gain, gate_master, up_master, down_master, count):
    shape = (3, *gate_master.shape)
    anywhere = pl.BlockSpec(memory_space=pltpu.HBM)
    return pl.pallas_call(
        copies_kernel,
        out_shape=jax.ShapeDtypeStruct((count, *shape), jnp.bfloat16),
        in_specs=[anywhere] * 4,
        out_specs=anywhere,
        scratch_shapes=[
            pltpu.VMEM((1, norm_gain.shape[0]), jnp.float32),
            pltpu.VMEM(shape, jnp.float32),
            pltpu.VMEM(shape, jnp.bfloat16),
            pltpu.SemaphoreType.DMA((4,)),
            pltpu.SemaphoreType.DMA((count,)),
        ],
        compiler_params=pltpu.CompilerParams(vmem_limit_bytes=66846720),
        cost_estimate=pl.CostEstimate(flops=1000000, bytes_accessed=4000000, transcendentals=0),
        name="prepare",
    )(norm_gain.reshape(1, -1), gate_master, up_master, down_master)


def blocks_of(ref, by, order):
    rows = ref.shape[0] // 4
    plane = lax.rem(lax.axis_index("zh") * 4 + lax.axis_index("zl") + by + 16, 16)
    first = lax.div(plane, 4)
    return [ref[pl.ds(pl.multiple_of(lax.rem(first + j, 4) * rows, rows), rows)] for j in order]


def blocks_of_twos(ref):
    up = lax.axis_index("c") == 0
    return blocks_of(ref, jnp.where(up, 2, -2), [jnp.where(up, a, b) for a, b in ((0, 1), (1, 2), (3, 0), (2, 3))])


def sums_kernel(orders, *refs):
    count = len(orders)
    rows_refs, (own_ref, partner_ref), out_refs = refs[:count], refs[count : count + 2], refs[count + 2 :]
    rows = jnp.concatenate([block for order, ref in zip(orders, rows_refs) for block in order(ref)], axis=0)
    width = rows.shape[1]
    wide = rows.astype(jnp.float32)
    row_scale = lax.rsqrt(jnp.mean(wide * wide, axis=1, keepdims=True) + 1e-06)
    hidden = []
    for ref in (own_ref, partner_ref):
        gate = ref[:, 0].reshape(width, -1)
        up = ref[:, 1].reshape(width, -1)
        gate_proj = row_scale * jnp.dot(rows, gate, preferred_element_type=jnp.float32)
        up_proj = row_scale * jnp.dot(rows, up, preferred_element_type=jnp.float32)
        hidden.append((gate_proj / (1.0 + jnp.exp(-gate_proj)) * up_proj).astype(jnp.bfloat16))
    total = None
    for ref, part in zip((own_ref, partner_ref), hidden):
        down = ref[:, 2].reshape(width, -1)
        share = lax.dot_general(part, down, (((1,), (1,)), ((), ())), preferred_element_type=jnp.float32)
        total = share if total is None else total + share
    at = 0
    for ref in out_refs:
        ref[...] = total[at : at + ref.shape[0]].astype(ref.dtype)
        at += ref.shape[0]


def partial_sums(parts, orders, weights, counts, dtypes):
    units = 2 * weights[0].shape[-1]
    count, width = sum(counts), parts[0].shape[1]
    return local(
        lambda *refs: sums_kernel(orders, *refs),
        tuple(jax.ShapeDtypeStruct((k, width), dtype) for k, dtype in zip(counts, dtypes)),
        *parts,
        *weights,
        flops=6 * count * width * units,
        transcendentals=count * units,
    )


def fold_far_kernel(own_ref, next_ref, prev_ref, far_ref):
    rows = far_ref.shape[0]
    total = own_ref[rows : 2 * rows]
    for other in (next_ref, prev_ref):
        total = total + other[rows : 2 * rows].astype(jnp.float32)
    far_ref[...] = total.astype(far_ref.dtype)


def fold_near_kernel(way, own_ref, next_ref, prev_ref, next2_ref, prev2_ref, *refs):
    *far_refs, out_ref = refs
    rows = out_ref.shape[0]
    up = lax.axis_index("c") == way
    lower = pl.multiple_of(jnp.where(up, 2, 3) * rows, rows)
    total = own_ref[pl.ds(lower, rows)] + jnp.where(up, next2_ref[rows:].astype(jnp.float32), prev2_ref[rows:].astype(jnp.float32))
    for other in (next_ref, prev_ref):
        total = total + other[pl.ds(lower, rows)].astype(jnp.float32)
    for ref in far_refs:
        total = total + ref[...].astype(jnp.float32)
    out_ref[...] = total.astype(out_ref.dtype)


def mix_kernel(tokens_ref, own_ref, next_ref, prev_ref, next2_ref, prev2_ref, above_ref, below_ref, out_ref):
    rows = tokens_ref.shape[0]
    total = own_ref[:rows]
    for ref in (next_ref, prev_ref, next2_ref, prev2_ref, above_ref, below_ref):
        total = total + ref[:rows].astype(jnp.float32)
    out_ref[...] = (tokens_ref[...].astype(jnp.float32) + 0.5 * total).astype(out_ref.dtype)


def step(tokens, norm_gain, gate_master, up_master, down_master):
    copies = weight_copies(norm_gain, gate_master, up_master, down_master, lax.axis_size("fs"))
    packed = lax.all_to_all(copies, "fs", split_axis=0, concat_axis=0, tiled=True)
    held = lax.all_gather(tokens, "zh", axis=0, tiled=True)
    rows, width = tokens.shape
    from_next = move(held, -1)
    from_prev = move(held, 1)
    from_twos = move_by_core(held, -2)

    partner = lax.ppermute(packed, "c", [(0, 1), (1, 0)])
    weights = (packed, partner)

    def around(by):
        return lambda ref: blocks_of(ref, by, (0, 2, 1, 3))

    narrow = jnp.bfloat16
    for_next, for_prev, own = partial_sums(
        (from_next, from_prev, held), (around(1), around(-1), around(0)), weights, (4 * rows,) * 3, (narrow, narrow, jnp.float32)
    )
    to_next = move(for_next, 1)
    to_prev = move(for_prev, -1)
    for_next2, for_prev2 = partial_sums((from_twos,), (blocks_of_twos,), weights, (2 * rows,) * 2, (narrow, narrow))
    to_prev2 = move(for_prev2, -2)
    to_next2 = move(for_next2, 2)

    block = jax.ShapeDtypeStruct((rows, width), jnp.bfloat16)
    (sum_far,) = local(fold_far_kernel, (block,), own, to_next, to_prev)
    back_far = move_by_core(sum_far, 4)
    received = (own, to_next, to_prev, to_next2, to_prev2)
    (sum_plain,) = local(lambda *refs: fold_near_kernel(1, *refs), (block,), *received)
    back_plain = move_by_core(sum_plain, -4)
    (sum_joint,) = local(lambda *refs: fold_near_kernel(0, *refs), (block,), *received, back_far)
    back_joint = move_by_core(sum_joint, 4)
    (mixed,) = local(mix_kernel, (block,), tokens, *received, back_plain, back_joint)
    return (mixed, *(packed[:, k].reshape(-1, packed.shape[-1]) for k in range(3)))


def solution(mesh):
    split = Mesh(mesh.devices.reshape(mesh.shape["fs"], 4, 4, 2), ROWS)
    placed = (P(ROWS, None), P("fs"), P("fs", TP), P("fs", TP), P("fs", TP))
    return jax.shard_map(
        step,
        mesh=split,
        in_specs=placed,
        out_specs=(P(ROWS, None), P(None, TP), P(None, TP), P(None, TP)),
        check_vma=False,
    )
```

```python
import jax
import jax.numpy as jnp
from jax import lax
from jax.experimental import pallas as pl
from jax.experimental.pallas import tpu as pltpu
from jax.sharding import Mesh
from jax.sharding import PartitionSpec as P


Z = ("zh", "zl")
TP = (*Z, "c")
ROWS = ("fs", *TP)
VMEM = pl.BlockSpec(memory_space=pltpu.VMEM)
PARAMS = pltpu.CompilerParams(vmem_limit_bytes=32 * 1024 * 1024)


def local(kernel, outs, *args, flops=0, transcendentals=0):
    moved = sum(a.size * a.dtype.itemsize for a in (*args, *outs))
    return pl.pallas_call(
        kernel,
        out_shape=outs,
        in_specs=[VMEM] * len(args),
        out_specs=tuple(VMEM for _ in outs),
        compiler_params=PARAMS,
        cost_estimate=pl.CostEstimate(flops=flops, bytes_accessed=moved, transcendentals=transcendentals),
    )(*args)


def move(array, by):
    planes = lax.axis_size(Z)
    return lax.ppermute(array, Z, [(i, (i + by) % planes) for i in range(planes)])


def move_by_core(array, by):
    planes = lax.axis_size(Z)
    pairs = [(2 * i + c, 2 * ((i + way * by) % planes) + c) for c, way in ((0, 1), (1, -1)) for i in range(planes)]
    return lax.ppermute(array, TP, pairs)


def copies_kernel(gain_hbm, gate_hbm, up_hbm, down_hbm, out_hbm, gain_ref, wide_ref, shard_ref, in_sems, out_sems):
    loads = [pltpu.make_async_copy(gain_hbm, gain_ref, in_sems.at[3])]
    for k, source in enumerate((gate_hbm, up_hbm, down_hbm)):
        loads.append(pltpu.make_async_copy(source, wide_ref.at[k], in_sems.at[k]))
    for load in loads:
        load.start()
    loads[0].wait()
    count = gate_hbm.shape[0]
    gain = jnp.transpose(jnp.broadcast_to(gain_ref[...], (count, count)))
    gain = jnp.concatenate([gain] * (gate_hbm.shape[1] // count), axis=1)
    stores = []
    for k in range(3):
        loads[1 + k].wait()
        value = wide_ref[k]
        shard_ref[k] = (value if k == 2 else gain * value).astype(jnp.bfloat16)
    for i in range(out_hbm.shape[0]):
        stores.append(pltpu.make_async_copy(shard_ref, out_hbm.at[i], out_sems.at[i]))
        stores[-1].start()
    for store in stores:
        store.wait()


def weight_copies(norm_gain, gate_master, up_master, down_master, count):
    shape = (3, *gate_master.shape)
    anywhere = pl.BlockSpec(memory_space=pltpu.HBM)
    return pl.pallas_call(
        copies_kernel,
        out_shape=jax.ShapeDtypeStruct((count, *shape), jnp.bfloat16),
        in_specs=[anywhere] * 4,
        out_specs=anywhere,
        scratch_shapes=[
            pltpu.VMEM((1, norm_gain.shape[0]), jnp.float32),
            pltpu.VMEM(shape, jnp.float32),
            pltpu.VMEM(shape, jnp.bfloat16),
            pltpu.SemaphoreType.DMA((4,)),
            pltpu.SemaphoreType.DMA((count,)),
        ],
        compiler_params=pltpu.CompilerParams(vmem_limit_bytes=66846720),
        cost_estimate=pl.CostEstimate(flops=1000000, bytes_accessed=4000000, transcendentals=0),
        name="prepare",
    )(norm_gain.reshape(1, -1), gate_master, up_master, down_master)


def blocks_of(ref, by, order):
    rows = ref.shape[0] // 4
    plane = lax.rem(lax.axis_index("zh") * 4 + lax.axis_index("zl") + by + 16, 16)
    first = lax.div(plane, 4)
    return [ref[pl.ds(pl.multiple_of(lax.rem(first + j, 4) * rows, rows), rows)] for j in order]


def blocks_of_twos(ref):
    up = lax.axis_index("c") == 0
    return blocks_of(ref, jnp.where(up, 2, -2), [jnp.where(up, a, b) for a, b in ((0, 1), (1, 2), (3, 0), (2, 3))])


def sums_kernel(orders, *refs):
    count = len(orders)
    rows_refs, (own_ref, partner_ref), out_refs = refs[:count], refs[count : count + 2], refs[count + 2 :]
    rows = jnp.concatenate([block for order, ref in zip(orders, rows_refs) for block in order(ref)], axis=0)
    width = rows.shape[1]
    wide = rows.astype(jnp.float32)
    row_scale = lax.rsqrt(jnp.mean(wide * wide, axis=1, keepdims=True) + 1e-06)
    hidden = []
    for ref in (own_ref, partner_ref):
        gate = ref[:, 0].reshape(width, -1)
        up = ref[:, 1].reshape(width, -1)
        gate_proj = row_scale * jnp.dot(rows, gate, preferred_element_type=jnp.float32)
        up_proj = row_scale * jnp.dot(rows, up, preferred_element_type=jnp.float32)
        hidden.append((gate_proj / (1.0 + jnp.exp(-gate_proj)) * up_proj).astype(jnp.bfloat16))
    total = None
    for ref, part in zip((own_ref, partner_ref), hidden):
        down = ref[:, 2].reshape(width, -1)
        share = lax.dot_general(part, down, (((1,), (1,)), ((), ())), preferred_element_type=jnp.float32)
        total = share if total is None else total + share
    at = 0
    for ref in out_refs:
        ref[...] = total[at : at + ref.shape[0]].astype(ref.dtype)
        at += ref.shape[0]


def partial_sums(parts, orders, weights, counts, dtype):
    units = 2 * weights[0].shape[-1]
    count, width = sum(counts), parts[0].shape[1]
    return local(
        lambda *refs: sums_kernel(orders, *refs),
        tuple(jax.ShapeDtypeStruct((k, width), dtype) for k in counts),
        *parts,
        *weights,
        flops=6 * count * width * units,
        transcendentals=count * units,
    )


def fold_far_kernel(own_ref, next_ref, prev_ref, far_ref):
    rows = far_ref.shape[0]
    total = own_ref[rows : 2 * rows]
    for other in (next_ref, prev_ref):
        total = total + other[rows : 2 * rows].astype(jnp.float32)
    far_ref[...] = total.astype(far_ref.dtype)


def fold_near_kernel(way, own_ref, next_ref, prev_ref, next2_ref, prev2_ref, *refs):
    *far_refs, out_ref = refs
    rows = out_ref.shape[0]
    up = lax.axis_index("c") == way
    lower = pl.multiple_of(jnp.where(up, 2, 3) * rows, rows)
    total = own_ref[pl.ds(lower, rows)] + jnp.where(up, next2_ref[rows:].astype(jnp.float32), prev2_ref[rows:].astype(jnp.float32))
    for other in (next_ref, prev_ref):
        total = total + other[pl.ds(lower, rows)].astype(jnp.float32)
    for ref in far_refs:
        total = total + ref[...].astype(jnp.float32)
    out_ref[...] = total.astype(out_ref.dtype)


def mix_kernel(tokens_ref, own_ref, next_ref, prev_ref, next2_ref, prev2_ref, above_ref, below_ref, out_ref):
    rows = tokens_ref.shape[0]
    total = own_ref[:rows]
    for ref in (next_ref, prev_ref, next2_ref, prev2_ref, above_ref, below_ref):
        total = total + ref[:rows].astype(jnp.float32)
    out_ref[...] = (tokens_ref[...].astype(jnp.float32) + 0.5 * total).astype(out_ref.dtype)


def step(tokens, norm_gain, gate_master, up_master, down_master):
    copies = weight_copies(norm_gain, gate_master, up_master, down_master, lax.axis_size("fs"))
    packed = lax.all_to_all(copies, "fs", split_axis=0, concat_axis=0, tiled=True)
    held = lax.all_gather(tokens, "zh", axis=0, tiled=True)
    rows, width = tokens.shape
    from_next = move(held, -1)
    from_prev = move(held, 1)
    from_twos = move_by_core(held, -2)

    partner = lax.ppermute(packed, "c", [(0, 1), (1, 0)])
    weights = (packed, partner)

    def around(by):
        return lambda ref: blocks_of(ref, by, (0, 2, 1, 3))

    (for_next,) = partial_sums((from_next,), (around(1),), weights, (4 * rows,), jnp.bfloat16)
    to_next = move(for_next, 1)
    (for_prev,) = partial_sums((from_prev,), (around(-1),), weights, (4 * rows,), jnp.bfloat16)
    to_prev = move(for_prev, -1)
    for_next2, for_prev2 = partial_sums((from_twos,), (blocks_of_twos,), weights, (2 * rows, 2 * rows), jnp.bfloat16)
    to_next2 = move(for_next2, 2)
    to_prev2 = move(for_prev2, -2)
    (own,) = partial_sums((held,), (around(0),), weights, (4 * rows,), jnp.float32)

    block = jax.ShapeDtypeStruct((rows, width), jnp.bfloat16)
    (sum_far,) = local(fold_far_kernel, (block,), own, to_next, to_prev)
    back_far = move_by_core(sum_far, 4)
    received = (own, to_next, to_prev, to_next2, to_prev2)
    (sum_plain,) = local(lambda *refs: fold_near_kernel(1, *refs), (block,), *received)
    back_plain = move_by_core(sum_plain, -4)
    (sum_joint,) = local(lambda *refs: fold_near_kernel(0, *refs), (block,), *received, back_far)
    back_joint = move_by_core(sum_joint, 4)
    (mixed,) = local(mix_kernel, (block,), tokens, *received, back_plain, back_joint)
    return (mixed, *(packed[:, k].reshape(-1, packed.shape[-1]) for k in range(3)))


def solution(mesh):
    split = Mesh(mesh.devices.reshape(mesh.shape["fs"], 4, 4, 2), ROWS)
    placed = (P(ROWS, None), P("fs"), P("fs", TP), P("fs", TP), P("fs", TP))
    return jax.shard_map(
        step,
        mesh=split,
        in_specs=placed,
        out_specs=(P(ROWS, None), P(None, TP), P(None, TP), P(None, TP)),
        check_vma=False,
    )
```
